32 devices in a mesh: fs: 16 (over z, y, x), tp: 2 (over core).
Axes of the slice: x: 2, y: 2, z: 4, core: 2. Of those that a mesh axis runs over, the one named last changes fastest.
Arguments:
- normed_input: bfloat16 [8192, 4096], P('fs', 'tp'), may hold values from -6 to 6
- value_cotangent: bfloat16 [8192, 2048], P('fs', 'tp'), may hold values from -0.01171875 to 0.01171875
- mixer_output: bfloat16 [8192, 2048], P('fs', 'tp'), may hold values from -6 to 6
- output_cotangent: bfloat16 [8192, 4096], P('fs', 'tp'), may hold values from -0.015625 to 0.015625
- value_factor: bfloat16 [4096, 128], replicated, may hold values from -0.5 to 0.5
- output_factor: bfloat16 [2048, 128], replicated, may hold values from -0.5 to 0.5
- value_master: float32 [4096, 2048], P('fs', 'tp'), may hold values from -0.09375 to 0.09375
- value_moment: float32 [128, 2048], P(None, 'tp'), may hold values from -6 to 6
- value_second: float32 [128, 2048], P(None, 'tp'), may hold values from 0.0625 to 16, as said below
- output_master: float32 [2048, 4096], P('fs', 'tp'), may hold values from -0.125 to 0.125
- output_moment: float32 [128, 4096], P(None, 'tp'), may hold values from -6 to 6
- output_second: float32 [128, 4096], P(None, 'tp'), may hold values from 0.0625 to 16, as said below
Outputs:
- value_step: float32 [4096, 2048], P('fs', 'tp')
- value_new: float32 [4096, 2048], P('fs', 'tp')
- value_copy: bfloat16 [4096, 2048], P(None, 'tp')
- value_moment_new: float32 [128, 2048], P(None, 'tp')
- value_second_new: float32 [128, 2048], P(None, 'tp')
- output_step: float32 [2048, 4096], P('fs', 'tp')
- output_new: float32 [2048, 4096], P('fs', 'tp')
- output_copy: bfloat16 [2048, 4096], P(None, 'tp')
- output_moment_new: float32 [128, 4096], P(None, 'tp')
- output_second_new: float32 [128, 4096], P(None, 'tp')
The draws below stay inside these ranges and needn't reach their ends.
Inputs may be any that keep to these rules, and one draw needn't show every extreme that they name: `value_second`: positive, with a scale that differs between groups of columns. `output_second`: positive, with a scale that differs between groups of columns.
All inputs are finite; a program needn't handle non-finite values.
Results may differ from the reference program's by a relative error of at most 0.004.
Values may be sent and summed in bfloat16 or wider, within the bound.
A program may use at most 128 MiB of HBM per device.

```python
import math
import jax
import jax.numpy as jnp
from jax import lax

D = 4096
WIDTH = 2048
R = 128
TOK_DEV = 512
TOKENS = 8192
N_FS = 16
N_TP = 2


def second_draw(key, rows, columns):
    levels = jnp.exp(jax.random.uniform(jax.random.fold_in(key, 11), (rows, columns), jnp.float32, math.log(0.25), math.log(4.0)))
    groups = jnp.exp(jax.random.uniform(jax.random.fold_in(key, 12), (16,), jnp.float32, math.log(0.25), math.log(4.0)))
    return levels * jnp.repeat(groups, columns // 16)[None, :]


def draw_value_second(key, part):
    return second_draw(jax.random.fold_in(key, 1), R, WIDTH)


def draw_output_second(key, part):
    return second_draw(jax.random.fold_in(key, 2), R, D)


def strengthened(array, rng, source, target, parts, factor):
    def block_of(axis_at):
        return (jnp.arange(array.shape[axis_at]) // (array.shape[axis_at] // parts)).reshape((-1,) + (1,) * (array.ndim - 1 - axis_at))

    near = jax.random.permutation(rng, parts)[block_of(target)]
    other_side = (block_of(target) + parts // 2) % parts
    return jnp.where((block_of(source) == near) | (block_of(source) == other_side), factor * array, array)


def block_levels(own_key, extent, split, least, top_value):
    def one(axis_at, parts):
        draws = jax.random.uniform(jax.random.fold_in(jax.random.fold_in(own_key, 6), axis_at), (parts,), jnp.float32, least / len(split), top_value / len(split))
        return jnp.repeat(jnp.exp(draws), extent[axis_at] // parts).reshape((-1,) + (1,) * (len(extent) - axis_at - 1))

    factor_of = one(*split[0])
    for cut in split[1:]:
        factor_of = factor_of * one(*cut)
    return factor_of


def noise(key, extent, width, reach, pieces=(), dtype=jnp.bfloat16):
    result = width * jax.random.normal(key, extent, jnp.float32)
    if pieces:
        result = result * block_levels(key, extent, pieces, -0.22, 0.18)
    return jnp.clip(result, -reach, reach).astype(dtype)


def gaussian_with(key, dims, scale, bound, shards, heavy, held_as=jnp.bfloat16):
    array = scale * jax.random.normal(key, dims, jnp.float32)
    if shards:
        array = array * block_levels(key, dims, shards, -0.22, 0.18)
    return jnp.clip(strengthened(array, jax.random.fold_in(key, 3), *heavy), -bound, bound).astype(held_as)


def setup_inputs(seed: int = 0) -> dict:
    streams_of = jax.random.split(jax.random.key(seed), 13)
    return {
        "normed_input": gaussian_with(streams_of[0], (TOKENS, D), 1.0, 6.0, ((0, 16), (1, 2)), (0, 1, 16, 2.0)),
        "value_cotangent": noise(streams_of[1], (TOKENS, WIDTH), ((R / (D * TOK_DEV * N_FS)) ** 0.5), 0.01171875, ((0, 16), (1, 2))),
        "mixer_output": noise(streams_of[2], (TOKENS, WIDTH), 1.0, 6.0, ((0, 16), (1, 2))),
        "output_cotangent": noise(streams_of[3], (TOKENS, D), ((R / (WIDTH * TOK_DEV * N_FS)) ** 0.5), 0.015625, ((0, 16), (1, 2))),
        "value_factor": noise(streams_of[4], (D, R), R ** -0.5, 0.5),
        "output_factor": noise(streams_of[5], (WIDTH, R), R ** -0.5, 0.5),
        "value_master": noise(streams_of[6], (D, WIDTH), D ** -0.5, 0.09375, ((0, 16), (1, 2)), jnp.float32),
        "value_moment": noise(streams_of[7], (R, WIDTH), 1.0, 6.0, ((1, 2),), jnp.float32),
        "value_second": draw_value_second(jax.random.fold_in(streams_of[12], 71), 0),
        "output_master": noise(streams_of[9], (WIDTH, D), WIDTH ** -0.5, 0.125, ((0, 16), (1, 2)), jnp.float32),
        "output_moment": noise(streams_of[10], (R, D), 1.0, 6.0, ((1, 2),), jnp.float32),
        "output_second": draw_output_second(jax.random.fold_in(streams_of[12], 71), 0),
    }


BETA_ONE = 0.8
BETA_TWO = 0.9
EPSILON = 1e-08
STEP_RATE = 0.005
FLOOR = 0.25

def moments(first, second, projected):
    first_new = BETA_ONE * first + (1.0 - BETA_ONE) * projected
    second_new = BETA_TWO * second + (1.0 - BETA_TWO) * projected * projected
    normalized = first_new / (jnp.sqrt(second_new) + EPSILON)
    return (first_new, second_new, normalized)

def reference(normed_input, value_cotangent, mixer_output, output_cotangent, value_factor, output_factor, value_master, value_moment, value_second, output_master, output_moment, output_second):
    highest = lax.Precision.HIGHEST
    input_reduced = jnp.dot(normed_input.astype(jnp.float32), value_factor.astype(jnp.float32), precision=highest)
    value_projected = jnp.dot(input_reduced.T, value_cotangent.astype(jnp.float32), precision=highest)
    split_cols = WIDTH // N_TP
    mixer_blocks = mixer_output.astype(jnp.float32).reshape(TOKENS, N_TP, split_cols)
    factor_blocks = output_factor.astype(jnp.float32).reshape(N_TP, split_cols, R)
    partials = jnp.einsum('tnc,ncr->ntr', mixer_blocks, factor_blocks, precision=highest).astype(jnp.bfloat16)
    partials = lax.optimization_barrier(partials)
    mixer_reduced = lax.optimization_barrier(jnp.sum(partials.astype(jnp.float32), axis=0)).astype(jnp.bfloat16)
    output_projected = jnp.dot(mixer_reduced.astype(jnp.float32).T, output_cotangent.astype(jnp.float32), precision=highest)
    value_moment_new, value_second_new, value_norm = moments(value_moment, value_second, value_projected)
    output_moment_new, output_second_new, output_norm = moments(output_moment, output_second, output_projected)
    value_scale = lax.rsqrt(jnp.mean(value_norm * value_norm) + FLOOR)
    output_scale = lax.rsqrt(jnp.mean(output_norm * output_norm) + FLOOR)
    value_step = value_scale * jnp.dot(value_factor.astype(jnp.float32), value_norm, precision=highest)
    output_step = output_scale * jnp.dot(output_factor.astype(jnp.float32), output_norm, precision=highest)
    value_new = value_master - STEP_RATE * value_step
    output_new = output_master - STEP_RATE * output_step
    return (value_step, value_new, value_new.astype(jnp.bfloat16), value_moment_new, value_second_new, output_step, output_new, output_new.astype(jnp.bfloat16), output_moment_new, output_second_new)
```

```python
import collections
import functools

import jax
import jax.numpy as jnp
from jax import lax
from jax.experimental import pallas as pl
from jax.experimental.pallas import tpu as pltpu
from jax.sharding import PartitionSpec as P

BETA_ONE = 0.8
BETA_TWO = 0.9
EPSILON = 1e-08
STEP_RATE = 0.005
FLOOR = 0.25

MESH = pl.DeviceIdType.MESH
A, B, UP, DOWN = range(4)
PLANE = 4
LATENCY = 3
LEAD = 1.25
FLIGHT = 1.75


def pieces_of(rows, cols):
    count = max(1, min(4, rows * cols * 2 // 131072))
    while rows % (16 * count):
        count -= 1
    return count


def classes_of(counts):
    out = []
    for array, count in enumerate(counts):
        for p in range(count):
            plane_first = count == 4 and p == 3
            out.append((array, p, plane_first, A if (p + array) % 2 == 0 else B))
    return out


def onward(n_z, classes, z, item, via):
    _, fa, fb, p = item
    _, _, plane_first, order = classes[p]
    up = [UP] if z < n_z - 1 else []
    down = [DOWN] if z > 0 else []
    if via is None:
        return [A, B] + up + down
    if via in (UP, DOWN):
        return (up if via == UP else down) + ([] if plane_first else [A, B])
    links = []
    if (fa, fb) == (1, 0) and order == A:
        links.append(B)
    if (fa, fb) == (0, 1) and order == B:
        links.append(A)
    return links + (up + down if plane_first else [])


def hops_left(n_z, classes, z, item, link):
    _, fa, fb, p = item
    _, _, plane_first, order = classes[p]
    if link in (UP, DOWN):
        return (n_z - 2 - z if link == UP else z - 1) + (0 if plane_first else 2)
    turn = 1 if link == order and (fa, fb) == (0, 0) else 0
    return turn + (max(n_z - 1 - z, z) if plane_first else 0)


def plan(n_z, classes, reserved):
    pool = collections.defaultdict(list)
    arriving = collections.defaultdict(list)
    sends = {z: [] for z in range(n_z)}
    takes = {z: [] for z in range(n_z)}
    busy = collections.defaultdict(int)
    for z in range(n_z):
        for p in range(len(classes)):
            item = (z, 0, 0, p)
            for link in onward(n_z, classes, z, item, None):
                pool[z, link].append((0, item))
    missing = n_z * (n_z * PLANE - 1) * len(classes)
    tick = 0
    while missing:
        for z, item, via in arriving.pop(tick, ()):
            for link in onward(n_z, classes, z, item, via):
                pool[z, link].append((tick, item))
        for z in range(n_z):
            toward = 1 if 2 * z < n_z else -1
            for link in range(4):
                held = [n for start, way, n in reserved if way == link and start == tick]
                if held:
                    busy[z, link] = tick + held[0]
                waiting = pool[z, link]
                if busy[z, link] > tick or not waiting:
                    continue
                best = max(
                    waiting,
                    key=lambda x: (
                        hops_left(n_z, classes, z, x[1], link),
                        -abs(x[1][0] - z),
                        (x[1][0] - z) * toward,
                        -x[1][3],
                        -x[0],
                        -x[1][1],
                        -x[1][2],
                    ),
                )
                waiting.remove(best)
                item = best[1]
                source, fa, fb, p = item
                sends[z].append((tick, link, item))
                if link == A:
                    there, got = z, (source, 1 - fa, fb, p)
                elif link == B:
                    there, got = z, (source, fa, 1 - fb, p)
                else:
                    there, got = z + (1 if link == UP else -1), item
                takes[there].append((tick, link, got))
                arriving[tick + LATENCY].append((there, got, link))
                busy[z, link] = tick + 1
                missing -= 1
        tick += 1
    return sends, takes


def mirrored(n_z, events):
    swap = {A: A, B: B, UP: DOWN, DOWN: UP}
    return sorted(
        (tick, swap[link], (n_z - 1 - s, fa, fb, p)) for tick, link, (s, fa, fb, p) in events
    )


def roles_of(n_z, sends, takes):
    pairs = n_z % 2 == 0 and all(
        sorted(x[z]) == mirrored(n_z, x[n_z - 1 - z])
        for x in (sends, takes)
        for z in range(n_z // 2)
    )
    roles = []
    for z in range(n_z // 2 if pairs else n_z):
        events = []
        done = {}
        for tick, link, (source, fa, fb, p) in sorted(takes[z]):
            item = (source - z, fa, fb, p)
            done[item] = tick + FLIGHT
            events.append((tick + FLIGHT, 0, "take", link, item))
        last = collections.defaultdict(float)
        for tick, link, (source, fa, fb, p) in sorted(sends[z]):
            item = (source - z, fa, fb, p)
            when = max(tick - LEAD, done.get(item, 0.0), last[link])
            if item not in done and tick <= 4:
                when = 0.0
            last[link] = when
            events.append((when, 1, "send", link, item))
            events.append((max(tick + 3.0, when + 2.0), 2, "sent", link, item))
        roles.append((sorted(events, key=lambda e: e[:2]), done))
    return pairs, roles


def levels_of(n_z, z):
    out = [0]
    for d in range(1, n_z):
        for offset in (d, -d):
            if 0 <= z + offset < n_z:
                out.append(offset)
    return out


def step_kernel(
    n_fs,
    n_tp,
    normed_hbm,
    mixer_hbm,
    value_cot_hbm,
    output_cot_hbm,
    value_factor_hbm,
    output_factor_hbm,
    value_moment_hbm,
    value_second_hbm,
    output_moment_hbm,
    output_second_hbm,
    value_master_hbm,
    output_master_hbm,
    value_step,
    value_new,
    value_copy,
    value_moment_new,
    value_second_new,
    output_step,
    output_new,
    output_copy,
    output_moment_new,
    output_second_new,
    normed,
    mixer,
    value_cot,
    output_cot,
    value_factor,
    output_factor,
    value_moment,
    value_second,
    output_moment,
    output_second,
    value_master,
    output_master,
    load_sem,
    value_all,
    output_all,
    input_ref,
    mixer_ref,
    near_in,
    near_mix,
    squares,
    near_squares,
    total,
    part,
    a_recv,
    b_part,
    b_recv,
    quarter,
    z_part,
    z_recv,
    shares,
    wide,
    high,
    low,
    near_send,
    near_recv,
    sum_send,
    sum_recv,
    share_send,
    share_recv,
    gather_send,
    gather_recv,
):
    f32, bf16 = jnp.float32, jnp.bfloat16
    me = lax.axis_index("fs")
    column = lax.axis_index("tp")
    n_z = n_fs // PLANE
    half = n_fs // 2
    here_a = lax.rem(me, 2)
    here_b = lax.rem(me // 2, 2)
    here_z = me // PLANE
    alls = (value_all, output_all)
    rows = total.shape[1]
    cols = (value_cot.shape[1], output_cot.shape[1])
    starts = (0, cols[0])
    classes = classes_of([x.shape[1] for x in alls])
    fine = len(classes) == 8

    if fine:
        reserved = (
            (4, A, 3),
            (9, B, 2),
            (13, UP, 2),
            (13, DOWN, 2),
            (17, UP, 2),
            (17, DOWN, 2),
            (21, A, 2),
            (25, B, 3),
        )
        stages = (7.8, 11.8, 15.8, 19.8, 23.8, 28.8)
    else:
        reserved = ()
        stages = tuple(7.8 + 4 * i for i in range(6))
    sends, takes = plan(n_z, classes, reserved)
    pairs, roles = roles_of(n_z, sends, takes)
    if pairs:
        toward = jnp.where(2 * here_z < n_z, 1, -1)
        role = jnp.where(2 * here_z < n_z, here_z, n_z - 1 - here_z)
    else:
        toward = 1
        role = here_z

    across_a = me + 1 - 2 * here_a
    across_b = me + 2 - 4 * here_b
    targets = {
        A: across_a,
        B: across_b,
        UP: me + toward * PLANE,
        DOWN: me - toward * PLANE,
    }
    places = {
        (fa, fb): (1 - here_b if fb else here_b) * 2 + (1 - here_a if fa else here_a)
        for fa in range(2)
        for fb in range(2)
    }

    def z_mate(k):
        return lax.rem(here_z + k, n_z) * PLANE + lax.rem(me, PLANE)

    barrier = pltpu.get_barrier_semaphore()
    for there in [across_a, across_b] + [z_mate(k) for k in range(1, n_z)]:
        pl.semaphore_signal(barrier, inc=1, device_id={"fs": there}, device_id_type=MESH)
    for k in range(1, n_tp):
        pl.semaphore_signal(
            barrier,
            inc=1,
            device_id={"tp": lax.rem(column + k, n_tp)},
            device_id_type=MESH,
        )

    loads = [
        pltpu.make_async_copy(src, dst, load_sem.at[i])
        for i, (src, dst) in enumerate(
            (
                (value_master_hbm, value_master),
                (output_master_hbm, output_master),
                (mixer_hbm, mixer),
                (output_factor_hbm, output_factor),
                (normed_hbm, normed),
                (value_factor_hbm, value_factor),
                (value_cot_hbm, value_cot),
                (output_cot_hbm, output_cot),
                (value_moment_hbm, value_moment),
                (value_second_hbm, value_second),
                (output_moment_hbm, output_moment),
                (output_second_hbm, output_second),
            )
        )
    ]
    for copy in loads:
        copy.start()
    for i, master in enumerate((value_master, output_master)):
        loads[i].wait()
        height = alls[i].shape[2]
        for p in range(alls[i].shape[1]):
            alls[i][me, p] = master[p * height : (p + 1) * height, :].astype(bf16)
    pl.semaphore_wait(barrier, 2 + (n_z - 1) + (n_tp - 1))

    def piece_copy(link, item):
        offset, fa, fb, p = item
        source = (here_z + toward * offset) * PLANE + places[fa, fb]
        array, piece, _, _ = classes[p]
        there = alls[array].at[source, piece]
        return pltpu.make_async_remote_copy(
            src_ref=there,
            dst_ref=there,
            send_sem=gather_send.at[link, source, p],
            recv_sem=gather_recv.at[source, p],
            device_id={"fs": targets[link]},
            device_id_type=MESH,
        )

    def run_events(k, first, last):
        events = [e for e in roles[k][0] if first <= e[0] < last]
        if not events:
            return

        @pl.when(role == k)
        def _():
            for _, _, kind, link, item in events:
                copy = piece_copy(link, item)
                if kind == "take":
                    copy.wait_recv()
                elif kind == "send":
                    copy.start()
                else:
                    copy.wait_send()

    def message(src, dst, there, sems, index):
        send, recv = sems
        return pltpu.make_async_remote_copy(
            src_ref=src,
            dst_ref=dst,
            send_sem=send.at[index],
            recv_sem=recv.at[index],
            device_id={"fs": there},
            device_id_type=MESH,
        )

    sums = (sum_send, sum_recv)
    shared = (share_send, share_recv)
    pending = []

    def start(copies):
        for copy in copies:
            copy.start()
        pending.extend(copies)
        return copies

    a_sum = message(part.at[pl.ds((1 - here_a) * half, half)], a_recv, across_a, sums, 0)
    b_sum = message(b_part, b_recv, across_b, sums, n_z)
    z_sums = [
        message(z_part.at[lax.rem(here_z + k, n_z)], z_recv.at[k], z_mate(k), sums, k)
        for k in range(1, n_z)
    ]
    mine = here_a * half + here_b * n_z
    z_shares = [
        message(shares.at[mine + here_z], shares.at[mine + here_z], z_mate(k), shared, k)
        for k in range(1, n_z)
    ]
    ours = shares.at[pl.ds(mine, n_z)]
    other = shares.at[pl.ds((1 - here_a) * half + here_b * n_z, n_z)]
    a_share = message(ours, ours, across_a, shared, 0)
    b_shares = [
        message(ours, ours, across_b, shared, n_z),
        message(other, other, across_b, shared, n_z + 1),
    ]

    def products():
        near = []
        for i, (tokens, factor, own, dst) in enumerate(
            (
                (mixer, output_factor, mixer_ref, near_mix),
                (normed, value_factor, input_ref, near_in),
            )
        ):
            loads[2 + 2 * i].wait()
            loads[3 + 2 * i].wait()
            depth = tokens.shape[1]
            rows_here = factor[pl.ds(pl.multiple_of(column * depth, depth), depth), :]
            own[...] = jnp.dot(
                tokens[...], rows_here, preferred_element_type=f32
            ).astype(bf16)
            for k in range(1, n_tp):
                copy = pltpu.make_async_remote_copy(
                    src_ref=own,
                    dst_ref=dst.at[k - 1],
                    send_sem=near_send.at[k - 1, i],
                    recv_sem=near_recv.at[k - 1, i],
                    device_id={"tp": lax.rem(column + k, n_tp)},
                    device_id_type=MESH,
                )
                copy.start()
                near.append(copy)
        for copy in near:
            copy.wait()
        input_total = input_ref[...].astype(f32)
        mixer_total = mixer_ref[...].astype(f32)
        for k in range(n_tp - 1):
            input_total += near_in[k].astype(f32)
            mixer_total += near_mix[k].astype(f32)
        for copy in loads[6:8]:
            copy.wait()
        across = (((0,), (0,)), ((), ()))
        for i, (left, right) in enumerate(
            (
                (input_total.astype(bf16), value_cot),
                (mixer_total.astype(bf16), output_cot),
            )
        ):
            tile = 512 if cols[i] % 512 == 0 else cols[i]
            for c in range(cols[i] // tile):
                product = lax.dot_general(
                    left,
                    right[:, c * tile : (c + 1) * tile],
                    across,
                    preferred_element_type=f32,
                )
                at = slice(starts[i] + c * tile, starts[i] + (c + 1) * tile)
                for s in range(n_fs):
                    block = product[s * rows : (s + 1) * rows]
                    total[s, :, at] = block
                    part[s, :, at] = block.astype(bf16)
        start([a_sum])

    def second_sum():
        a_sum.wait_recv()
        away = (1 - here_b) * n_z
        b_part[...] = (
            total[pl.ds(here_a * half + away, n_z)] + a_recv[pl.ds(away, n_z)].astype(f32)
        ).astype(bf16)
        start([b_sum])
        quarter[...] = total[pl.ds(mine, n_z)] + a_recv[pl.ds(here_b * n_z, n_z)].astype(f32)

    def third_sum():
        b_sum.wait_recv()
        quarter[...] += b_recv[...].astype(f32)
        z_part[...] = quarter[...].astype(bf16)
        start(z_sums)

    def last_sum():
        for copy in z_sums:
            copy.wait_recv()
        done = quarter[here_z]
        for k in range(1, n_z):
            done += z_recv[k].astype(f32)
        shares[mine + here_z] = done.astype(bf16)
        start(z_shares)

    def share_a():
        for copy in z_shares:
            copy.wait_recv()
        start([a_share])

    def share_b():
        a_share.wait_recv()
        start(b_shares)

    square_copies = [
        pltpu.make_async_remote_copy(
            src_ref=squares,
            dst_ref=near_squares.at[k - 1],
            send_sem=near_send.at[k - 1, 2],
            recv_sem=near_recv.at[k - 1, 2],
            device_id={"tp": lax.rem(column + k, n_tp)},
            device_id_type=MESH,
        )
        for k in range(1, n_tp)
    ]
    rank = value_factor.shape[1]
    block = 16

    def moments():
        for copy in b_shares:
            copy.wait_recv()
        for copy in loads[8:]:
            copy.wait()
        for s in range(n_fs):
            wide[s * rows : (s + 1) * rows, :] = shares[s].astype(f32)
        for i, (first, second, first_new, second_new) in enumerate(
            (
                (value_moment, value_second, value_moment_new, value_second_new),
                (output_moment, output_second, output_moment_new, output_second_new),
            )
        ):
            span = slice(starts[i], starts[i] + cols[i])

            def body(r, gathered, first=first, second=second, first_new=first_new,
                     second_new=second_new, span=span, i=i):
                at = pl.ds(pl.multiple_of(r * block, block), block)
                projected = wide[at, span]
                m = BETA_ONE * first[at, :] + (1.0 - BETA_ONE) * projected
                v = BETA_TWO * second[at, :] + (1.0 - BETA_TWO) * projected * projected
                norm = m / (jnp.sqrt(v) + EPSILON)
                first_new[at, :] = m
                second_new[at, :] = v
                wide[at, span] = norm
                square = norm * norm
                square = square[:8] + square[8:]
                for c in range(cols[i] // 128):
                    gathered += square[:, c * 128 : (c + 1) * 128]
                return gathered

            squares[i] = lax.fori_loop(
                0, rank // block, body, jnp.zeros((8, 128), f32)
            )
        for copy in square_copies:
            copy.start()

    def steps():
        for copy in square_copies:
            copy.wait()
        for i, (factor, master, step, new) in enumerate(
            (
                (value_factor, value_master, value_step, value_new),
                (output_factor, output_master, output_step, output_new),
            )
        ):
            gathered = squares[i]
            for k in range(n_tp - 1):
                gathered += near_squares[k, i]
            gathered = jnp.sum(jnp.sum(gathered, axis=1, keepdims=True), axis=0, keepdims=True)
            scale = lax.rsqrt(gathered / (rank * cols[i] * n_tp) + FLOOR)
            span = slice(starts[i], starts[i] + cols[i])

            def body(r, carry, span=span, scale=scale, width=cols[i]):
                at = pl.ds(pl.multiple_of(r * block, block), block)
                scaled = wide[at, span] * jnp.broadcast_to(scale, (block, width))
                rounded = scaled.astype(bf16)
                high[at, span] = rounded
                low[at, span] = (scaled - rounded.astype(f32)).astype(bf16)
                return carry

            lax.fori_loop(0, rank // block, body, 0)
            height = master.shape[0]
            here = factor[pl.ds(pl.multiple_of(me * height, height), height), :]
            tile = 512 if cols[i] % 512 == 0 else cols[i]
            for c in range(cols[i] // tile):
                at = slice(c * tile, (c + 1) * tile)
                inner = slice(starts[i] + c * tile, starts[i] + (c + 1) * tile)
                moved = jnp.dot(here, high[:, inner], preferred_element_type=f32) + jnp.dot(
                    here, low[:, inner], preferred_element_type=f32
                )
                step[:, at] = moved
                new[:, at] = master[:, at] - STEP_RATE * moved

    def copies(level, i, pieces):
        if pairs:
            offset = jnp.int32(0)
            for k in range(len(roles)):
                offset = jnp.where(role == k, levels_of(n_z, k)[level], offset)
            source_z = here_z + toward * offset
        else:
            offset = jnp.int32(0)
            for k in range(len(roles)):
                offset = jnp.where(role == k, levels_of(n_z, k)[level], offset)
            source_z = here_z + offset
        factor = (value_factor, output_factor)[i]
        out = (value_copy, output_copy)[i]
        height = alls[i].shape[2]
        tall = alls[i].shape[1] * height
        tile = 512 if cols[i] % 512 == 0 else cols[i]

        def body(c, carry):
            source = source_z * PLANE + c
            base = pl.multiple_of(source * tall, tall) + pieces[0] * height
            base = pl.multiple_of(base, height)
            here = factor[pl.ds(base, len(pieces) * height), :]
            for t in range(cols[i] // tile):
                at = slice(t * tile, (t + 1) * tile)
                inner = slice(starts[i] + t * tile, starts[i] + (t + 1) * tile)
                moved = jnp.dot(here, high[:, inner], preferred_element_type=f32)
                for n, p in enumerate(pieces):
                    old = alls[i][source, p, :, at].astype(f32)
                    fresh = old - STEP_RATE * moved[n * height : (n + 1) * height]
                    out[pl.ds(pl.multiple_of(base + n * height, height), height), at] = (
                        fresh.astype(bf16)
                    )
            return carry

        lax.fori_loop(0, PLANE, body, 0)

    work = [
        (0.5, products),
        (stages[0], second_sum),
        (stages[1], third_sum),
        (stages[2], last_sum),
        (stages[3], share_a),
        (stages[4], share_b),
        (stages[5], moments),
        (stages[5] + 0.5, steps),
    ]
    free = stages[5] + 0.6
    ready = []
    for level in range(n_z):
        for i in range(2):
            count = alls[i].shape[1]
            groups = [tuple(range(count))]
            if level == n_z - 1:
                groups = [(p,) for p in range(count)]
            for pieces in groups:
                when = 0.0
                for k in range(len(roles)):
                    offset = levels_of(n_z, k)[level]
                    for item, at in roles[k][1].items():
                        array, p, _, _ = classes[item[3]]
                        if item[0] == offset and array == i and p in pieces:
                            when = max(when, at)
                ready.append((when, len(ready), level, i, pieces))
    for when, _, level, i, pieces in sorted(ready):
        free = max(free + 0.45 * len(pieces) / alls[i].shape[1], when + 0.01)
        work.append((free, functools.partial(copies, level, i, pieces)))

    before = -1.0
    for when, action in sorted(work, key=lambda x: x[0]):
        for k in range(len(roles)):
            run_events(k, before, when)
        action()
        before = when
    for k in range(len(roles)):
        run_events(k, before, float("inf"))
    for copy in pending:
        copy.wait_send()


def per_device(
    n_fs,
    n_tp,
    normed_input,
    value_cotangent,
    mixer_output,
    output_cotangent,
    value_factor,
    output_factor,
    value_master,
    value_moment,
    value_second,
    output_master,
    output_moment,
    output_second,
):
    f32, bf16 = jnp.float32, jnp.bfloat16
    rank = value_factor.shape[1]
    rows = rank // n_fs
    n_z = n_fs // PLANE
    tokens, value_cols = value_cotangent.shape
    output_cols = output_cotangent.shape[1]
    both = value_cols + output_cols
    others = max(n_tp - 1, 1)
    dma = pltpu.SemaphoreType.DMA
    stacks = []
    for master in (value_master, output_master):
        count = pieces_of(*master.shape)
        stacks.append((n_fs, count, master.shape[0] // count, master.shape[1]))
    n_pieces = stacks[0][1] + stacks[1][1]
    streamed = (
        normed_input,
        mixer_output,
        value_cotangent,
        output_cotangent,
        value_factor,
        output_factor,
        value_moment,
        value_second,
        output_moment,
        output_second,
        value_master,
        output_master,
    )
    outs = []
    for master, moment in ((value_master, value_moment), (output_master, output_moment)):
        outs += [
            (master.shape, f32),
            (master.shape, f32),
            ((n_fs * master.shape[0], master.shape[1]), bf16),
            (moment.shape, f32),
            (moment.shape, f32),
        ]
    return pl.pallas_call(
        functools.partial(step_kernel, n_fs, n_tp),
        out_shape=tuple(pltpu.VMEM(*x) for x in outs),
        in_specs=[pl.BlockSpec(memory_space=pltpu.HBM)] * len(streamed),
        out_specs=(pl.BlockSpec(memory_space=pltpu.VMEM),) * len(outs),
        scratch_shapes=[pltpu.VMEM(x.shape, x.dtype) for x in streamed]
        + [
            dma((len(streamed),)),
            pltpu.VMEM(stacks[0], bf16),
            pltpu.VMEM(stacks[1], bf16),
            pltpu.VMEM((tokens, rank), bf16),
            pltpu.VMEM((tokens, rank), bf16),
            pltpu.VMEM((others, tokens, rank), bf16),
            pltpu.VMEM((others, tokens, rank), bf16),
            pltpu.VMEM((2, 8, 128), f32),
            pltpu.VMEM((others, 2, 8, 128), f32),
            pltpu.VMEM((n_fs, rows, both), f32),
            pltpu.VMEM((n_fs, rows, both), bf16),
            pltpu.VMEM((n_fs // 2, rows, both), bf16),
            pltpu.VMEM((n_z, rows, both), bf16),
            pltpu.VMEM((n_z, rows, both), bf16),
            pltpu.VMEM((n_z, rows, both), f32),
            pltpu.VMEM((n_z, rows, both), bf16),
            pltpu.VMEM((n_z, rows, both), bf16),
            pltpu.VMEM((n_fs, rows, both), bf16),
            pltpu.VMEM((rank, both), f32),
            pltpu.VMEM((rank, both), bf16),
            pltpu.VMEM((rank, both), bf16),
            dma((others, 3)),
            dma((others, 3)),
            dma((n_z + 1,)),
            dma((n_z + 1,)),
            dma((n_z + 2,)),
            dma((n_z + 2,)),
            dma((4, n_fs, n_pieces)),
            dma((n_fs, n_pieces)),
        ],
        compiler_params=pltpu.CompilerParams(
            collective_id=0, has_side_effects=True, vmem_limit_bytes=39 << 20
        ),
    )(*streamed)


def solution(mesh):
    return jax.shard_map(
        functools.partial(per_device, mesh.shape["fs"], mesh.shape["tp"]),
        mesh=mesh,
        in_specs=(
            P("fs", "tp"),
            P("fs", "tp"),
            P("fs", "tp"),
            P("fs", "tp"),
            P(),
            P(),
            P("fs", "tp"),
            P(None, "tp"),
            P(None, "tp"),
            P("fs", "tp"),
            P(None, "tp"),
            P(None, "tp"),
        ),
        out_specs=(
            P("fs", "tp"),
            P("fs", "tp"),
            P(None, "tp"),
            P(None, "tp"),
            P(None, "tp"),
            P("fs", "tp"),
            P("fs", "tp"),
            P(None, "tp"),
            P(None, "tp"),
            P(None, "tp"),
        ),
        check_vma=False,
    )
```

```python
import collections
import functools
import math

import jax
import jax.numpy as jnp
from jax import lax
from jax.experimental import pallas as pl
from jax.experimental.pallas import tpu as pltpu
from jax.sharding import PartitionSpec as P

BETA_ONE = 0.8
BETA_TWO = 0.9
EPSILON = 1e-08
STEP_RATE = 0.005
FLOOR = 0.25

MESH = pl.DeviceIdType.MESH
A, B, UP, DOWN = range(4)
PLANE = 4
GRAIN = 1
LATENCY = 6
LEAD = 3.0
FLIGHT = 1.75


def pieces_of(rows, cols):
    count = max(1, min(4 * GRAIN, rows * cols * 2 * GRAIN // 131072))
    while rows % (16 * count):
        count -= 1
    return count


def classes_of(counts):
    out = []
    for array, count in enumerate(counts):
        for p in range(count):
            plane_first = count % 4 == 0 and p % 4 == 3
            out.append((array, p, plane_first, A if (p + array) % 2 == 0 else B))
    return out


def onward(n_z, classes, z, item, via):
    _, fa, fb, p = item
    _, _, plane_first, order = classes[p]
    up = [UP] if z < n_z - 1 else []
    down = [DOWN] if z > 0 else []
    if via is None:
        return [A, B] + up + down
    if via in (UP, DOWN):
        return (up if via == UP else down) + ([] if plane_first else [A, B])
    links = []
    if (fa, fb) == (1, 0) and order == A:
        links.append(B)
    if (fa, fb) == (0, 1) and order == B:
        links.append(A)
    return links + (up + down if plane_first else [])


def hops_left(n_z, classes, z, item, link):
    _, fa, fb, p = item
    _, _, plane_first, order = classes[p]
    if link in (UP, DOWN):
        return (n_z - 2 - z if link == UP else z - 1) + (0 if plane_first else 2)
    turn = 1 if link == order and (fa, fb) == (0, 0) else 0
    return turn + (max(n_z - 1 - z, z) if plane_first else 0)


def plan(n_z, classes, reserved):
    pool = collections.defaultdict(list)
    arriving = collections.defaultdict(list)
    sends = {z: [] for z in range(n_z)}
    takes = {z: [] for z in range(n_z)}
    busy = collections.defaultdict(int)
    for z in range(n_z):
        for p in range(len(classes)):
            item = (z, 0, 0, p)
            for link in onward(n_z, classes, z, item, None):
                pool[z, link].append((0, item))
    missing = n_z * (n_z * PLANE - 1) * len(classes)
    tick = 0
    while missing:
        for z, item, via in arriving.pop(tick, ()):
            for link in onward(n_z, classes, z, item, via):
                pool[z, link].append((tick, item))
        for z in range(n_z):
            toward = 1 if 2 * z < n_z else -1
            for link in range(4):
                held = [
                    n * GRAIN
                    for start, way, n in reserved
                    if way == link and start * GRAIN == tick
                ]
                if held:
                    busy[z, link] = tick + held[0]
                waiting = pool[z, link]
                if busy[z, link] > tick or not waiting:
                    continue
                best = max(
                    waiting,
                    key=lambda x: (
                        hops_left(n_z, classes, z, x[1], link),
                        -abs(x[1][0] - z),
                        (x[1][0] - z) * toward,
                        -x[1][3],
                        -x[0],
                        -x[1][1],
                        -x[1][2],
                    ),
                )
                waiting.remove(best)
                item = best[1]
                source, fa, fb, p = item
                sends[z].append((tick, link, item))
                if link == A:
                    there, got = z, (source, 1 - fa, fb, p)
                elif link == B:
                    there, got = z, (source, fa, 1 - fb, p)
                else:
                    there, got = z + (1 if link == UP else -1), item
                takes[there].append((tick, link, got))
                arriving[tick + LATENCY * GRAIN].append((there, got, link))
                busy[z, link] = tick + 1
                missing -= 1
        tick += 1
    return sends, takes


def mirrored(n_z, events):
    swap = {A: A, B: B, UP: DOWN, DOWN: UP}
    return sorted(
        (tick, swap[link], (n_z - 1 - s, fa, fb, p)) for tick, link, (s, fa, fb, p) in events
    )


def roles_of(n_z, sends, takes):
    pairs = n_z % 2 == 0 and all(
        sorted(x[z]) == mirrored(n_z, x[n_z - 1 - z])
        for x in (sends, takes)
        for z in range(n_z // 2)
    )
    roles = []
    for z in range(n_z // 2 if pairs else n_z):
        events = []
        done = {}
        for tick, link, (source, fa, fb, p) in sorted(takes[z]):
            item = (source - z, fa, fb, p)
            done[item] = tick / GRAIN + FLIGHT
            events.append((done[item], 0, "take", link, item))
        last = collections.defaultdict(float)
        for tick, link, (source, fa, fb, p) in sorted(sends[z]):
            item = (source - z, fa, fb, p)
            at = tick / GRAIN
            when = max(at - LEAD, done.get(item, 0.0), last[link])
            if item not in done and at <= 4:
                when = 0.0
            last[link] = when
            events.append((when, 1, "send", link, item))
            events.append((max(at + 3.0, when + 2.0), 2, "sent", link, item))
        roles.append((sorted(events, key=lambda e: e[:2]), done))
    return pairs, roles


def levels_of(n_z, z):
    near, toward = (z, 1) if 2 * z < n_z else (n_z - 1 - z, -1)
    out = []
    for level in range(n_z):
        step = (level + 1) // 2 if level % 2 else -(level // 2)
        out.append(toward * (step if level <= 2 * near else level - near))
    return out


def level_z(n_z, here_z, level):
    near = jnp.where(2 * here_z < n_z, here_z, n_z - 1 - here_z)
    toward = jnp.where(2 * here_z < n_z, 1, -1)
    step = (level + 1) // 2 if level % 2 else -(level // 2)
    return here_z + toward * jnp.where(level <= 2 * near, step, level - near)


def renew(source_z, factor, high, start, old, out, first):
    _, count, height, cols = old.shape
    tall = count * height
    tile = 512 if cols % 512 == 0 else cols

    def body(c, carry):
        source = source_z * PLANE + c
        here = factor[pl.ds(pl.multiple_of(source * tall, tall), tall), :]
        for t in range(cols // tile):
            at = slice(t * tile, (t + 1) * tile)
            inner = slice(start + t * tile, start + (t + 1) * tile)
            moved = jnp.dot(here, high[:, inner], preferred_element_type=jnp.float32)
            for p in range(count):
                fresh = (
                    old[source, p, :, at].astype(jnp.float32)
                    - STEP_RATE * moved[p * height : (p + 1) * height]
                )
                out[first + c, p, :, at] = fresh.astype(jnp.bfloat16)
        return carry

    lax.fori_loop(0, PLANE, body, 0)


def step_kernel(
    n_fs,
    n_tp,
    normed_hbm,
    mixer_hbm,
    value_cot_hbm,
    output_cot_hbm,
    value_factor_hbm,
    output_factor_hbm,
    value_moment_hbm,
    value_second_hbm,
    output_moment_hbm,
    output_second_hbm,
    value_master_hbm,
    output_master_hbm,
    value_step,
    value_new,
    value_all,
    value_moment_new,
    value_second_new,
    output_step,
    output_new,
    output_all,
    output_moment_new,
    output_second_new,
    value_factor,
    output_factor,
    high,
    normed,
    mixer,
    value_cot,
    output_cot,
    value_moment,
    value_second,
    output_moment,
    output_second,
    value_master,
    output_master,
    load_sem,
    master_sem,
    input_ref,
    mixer_ref,
    near_in,
    near_mix,
    squares,
    near_squares,
    total,
    part,
    a_recv,
    b_part,
    b_recv,
    quarter,
    z_part,
    z_recv,
    shares,
    wide,
    low,
    near_send,
    near_recv,
    sum_send,
    sum_recv,
    share_send,
    share_recv,
    gather_send,
    gather_recv,
):
    f32, bf16 = jnp.float32, jnp.bfloat16
    me = lax.axis_index("fs")
    column = lax.axis_index("tp")
    n_z = n_fs // PLANE
    half = n_fs // 2
    here_a = lax.rem(me, 2)
    here_b = lax.rem(me // 2, 2)
    here_z = me // PLANE
    alls = (value_all, output_all)
    rows = total.shape[1]
    cols = (value_cot.shape[1], output_cot.shape[1])
    starts = (0, cols[0])
    classes = classes_of([x.shape[1] for x in alls])
    fine = len(classes) == 8 * GRAIN

    if fine:
        reserved = (
            (4, A, 3),
            (10, B, 2),
            (15, UP, 1),
            (15, DOWN, 1),
            (20, UP, 1),
            (20, DOWN, 1),
            (25, A, 2),
            (30, B, 3),
        )
        stages = (7.8, 12.8, 17.8, 22.8, 27.8, 33.8)
    else:
        reserved = ()
        stages = tuple(7.8 + 4 * i for i in range(6))
    sends, takes = plan(n_z, classes, reserved)
    pairs, roles = roles_of(n_z, sends, takes)
    if pairs:
        toward = jnp.where(2 * here_z < n_z, 1, -1)
        role = jnp.where(2 * here_z < n_z, here_z, n_z - 1 - here_z)
    else:
        toward = 1
        role = here_z

    across_a = me + 1 - 2 * here_a
    across_b = me + 2 - 4 * here_b
    targets = {
        A: across_a,
        B: across_b,
        UP: me + toward * PLANE,
        DOWN: me - toward * PLANE,
    }
    places = {
        (fa, fb): (1 - here_b if fb else here_b) * 2 + (1 - here_a if fa else here_a)
        for fa in range(2)
        for fb in range(2)
    }

    def z_mate(k):
        return lax.rem(here_z + k, n_z) * PLANE + lax.rem(me, PLANE)

    masters = []
    for array, p, _, _ in classes:
        hbm, master = ((value_master_hbm, value_master), (output_master_hbm, output_master))[array]
        height = alls[array].shape[2]
        at = pl.ds(p * height, height)
        masters.append(
            pltpu.make_async_copy(hbm.at[at], master.at[at], master_sem.at[len(masters)])
        )
    loads = [
        pltpu.make_async_copy(src, dst, load_sem.at[i])
        for i, (src, dst) in enumerate(
            (
                (mixer_hbm, mixer),
                (output_factor_hbm, output_factor),
                (normed_hbm, normed),
                (value_factor_hbm, value_factor),
                (value_cot_hbm, value_cot),
                (output_cot_hbm, output_cot),
                (value_moment_hbm, value_moment),
                (value_second_hbm, value_second),
                (output_moment_hbm, output_moment),
                (output_second_hbm, output_second),
            )
        )
    ]

    opening = [[] for _ in classes]
    for k, (events, _) in enumerate(roles):
        for when, _, kind, link, item in events:
            if kind == "send" and when == 0.0:
                opening[item[3]].append((k, link, item))
    queue = sorted(
        range(len(classes)),
        key=lambda p: min(
            [t for z in sends for t, _, item in sends[z] if item == (z, 0, 0, p)]
        ),
    )
    for p in queue:
        masters[p].start()

    barrier = pltpu.get_barrier_semaphore()
    for there in [across_a, across_b] + [z_mate(k) for k in range(1, n_z)]:
        pl.semaphore_signal(barrier, inc=1, device_id={"fs": there}, device_id_type=MESH)
    for k in range(1, n_tp):
        pl.semaphore_signal(
            barrier,
            inc=1,
            device_id={"tp": lax.rem(column + k, n_tp)},
            device_id_type=MESH,
        )

    def piece_copy(link, item):
        offset, fa, fb, p = item
        source = (here_z + toward * offset) * PLANE + places[fa, fb]
        array, piece, _, _ = classes[p]
        there = alls[array].at[source, piece]
        return pltpu.make_async_remote_copy(
            src_ref=there,
            dst_ref=there,
            send_sem=gather_send.at[link, source, p],
            recv_sem=gather_recv.at[source, p],
            device_id={"fs": targets[link]},
            device_id_type=MESH,
        )

    def open_piece(p):
        for k in range(len(roles)):
            out = [x for x in opening[p] if x[0] == k]
            if out:

                @pl.when(role == k)
                def _(out=out):
                    for _, link, item in out:
                        piece_copy(link, item).start()

    for n, p in enumerate(queue):
        masters[p].wait()
        array, piece, _, _ = classes[p]
        height = alls[array].shape[2]
        master = (value_master, output_master)[array]
        alls[array][me, piece] = master[piece * height : (piece + 1) * height, :].astype(bf16)
        if n == len(queue) - 1:
            for copy in loads:
                copy.start()
        if n == 0:
            pl.semaphore_wait(barrier, 2 + (n_z - 1) + (n_tp - 1))
        else:
            open_piece(queue[n - 1])
    open_piece(queue[-1])

    def run_events(k, first, last):
        events = [
            e for e in roles[k][0] if first <= e[0] < last and (e[2] != "send" or e[0] > 0.0)
        ]
        if not events:
            return

        @pl.when(role == k)
        def _():
            for _, _, kind, link, item in events:
                copy = piece_copy(link, item)
                if kind == "take":
                    copy.wait_recv()
                elif kind == "send":
                    copy.start()
                else:
                    copy.wait_send()

    def message(src, dst, there, sems, index):
        send, recv = sems
        return pltpu.make_async_remote_copy(
            src_ref=src,
            dst_ref=dst,
            send_sem=send.at[index],
            recv_sem=recv.at[index],
            device_id={"fs": there},
            device_id_type=MESH,
        )

    sums = (sum_send, sum_recv)
    shared = (share_send, share_recv)
    pending = []

    def start(copies):
        for copy in copies:
            copy.start()
        pending.extend(copies)
        return copies

    a_sum = message(part.at[pl.ds((1 - here_a) * half, half)], a_recv, across_a, sums, 0)
    b_sum = message(b_part, b_recv, across_b, sums, n_z)
    z_sums = [
        message(z_part.at[lax.rem(here_z + k, n_z)], z_recv.at[k], z_mate(k), sums, k)
        for k in range(1, n_z)
    ]
    mine = here_a * half + here_b * n_z
    z_shares = [
        message(shares.at[mine + here_z], shares.at[mine + here_z], z_mate(k), shared, k)
        for k in range(1, n_z)
    ]
    ours = shares.at[pl.ds(mine, n_z)]
    other = shares.at[pl.ds((1 - here_a) * half + here_b * n_z, n_z)]
    a_share = message(ours, ours, across_a, shared, 0)
    b_shares = [
        message(ours, ours, across_b, shared, n_z),
        message(other, other, across_b, shared, n_z + 1),
    ]

    def products():
        near = []
        for i, (tokens, factor, own, dst) in enumerate(
            (
                (mixer, output_factor, mixer_ref, near_mix),
                (normed, value_factor, input_ref, near_in),
            )
        ):
            loads[2 * i].wait()
            loads[2 * i + 1].wait()
            depth = tokens.shape[1]
            rows_here = factor[pl.ds(pl.multiple_of(column * depth, depth), depth), :]
            own[...] = jnp.dot(
                tokens[...], rows_here, preferred_element_type=f32
            ).astype(bf16)
            for k in range(1, n_tp):
                copy = pltpu.make_async_remote_copy(
                    src_ref=own,
                    dst_ref=dst.at[k - 1],
                    send_sem=near_send.at[k - 1, i],
                    recv_sem=near_recv.at[k - 1, i],
                    device_id={"tp": lax.rem(column + k, n_tp)},
                    device_id_type=MESH,
                )
                copy.start()
                near.append(copy)
        for copy in near:
            copy.wait()
        input_total = input_ref[...].astype(f32)
        mixer_total = mixer_ref[...].astype(f32)
        for k in range(n_tp - 1):
            input_total += near_in[k].astype(f32)
            mixer_total += near_mix[k].astype(f32)
        for copy in loads[4:6]:
            copy.wait()
        across = (((0,), (0,)), ((), ()))
        for i, (left, right) in enumerate(
            (
                (input_total.astype(bf16), value_cot),
                (mixer_total.astype(bf16), output_cot),
            )
        ):
            tile = 512 if cols[i] % 512 == 0 else cols[i]
            for c in range(cols[i] // tile):
                product = lax.dot_general(
                    left,
                    right[:, c * tile : (c + 1) * tile],
                    across,
                    preferred_element_type=f32,
                )
                at = slice(starts[i] + c * tile, starts[i] + (c + 1) * tile)
                for s in range(n_fs):
                    block = product[s * rows : (s + 1) * rows]
                    total[s, :, at] = block
                    part[s, :, at] = block.astype(bf16)
        start([a_sum])

    def second_sum():
        a_sum.wait_recv()
        away = (1 - here_b) * n_z
        b_part[...] = (
            total[pl.ds(here_a * half + away, n_z)] + a_recv[pl.ds(away, n_z)].astype(f32)
        ).astype(bf16)
        start([b_sum])
        quarter[...] = total[pl.ds(mine, n_z)] + a_recv[pl.ds(here_b * n_z, n_z)].astype(f32)

    def third_sum():
        b_sum.wait_recv()
        quarter[...] += b_recv[...].astype(f32)
        z_part[...] = quarter[...].astype(bf16)
        start(z_sums)

    def last_sum():
        for copy in z_sums:
            copy.wait_recv()
        done = quarter[here_z]
        for k in range(1, n_z):
            done += z_recv[k].astype(f32)
        shares[mine + here_z] = done.astype(bf16)
        start(z_shares)

    def share_a():
        for copy in z_shares:
            copy.wait_recv()
        start([a_share])

    def share_b():
        a_share.wait_recv()
        start(b_shares)

    square_copies = [
        pltpu.make_async_remote_copy(
            src_ref=squares,
            dst_ref=near_squares.at[k - 1],
            send_sem=near_send.at[k - 1, 2],
            recv_sem=near_recv.at[k - 1, 2],
            device_id={"tp": lax.rem(column + k, n_tp)},
            device_id_type=MESH,
        )
        for k in range(1, n_tp)
    ]
    rank = value_factor.shape[1]
    block = 16

    def moments():
        for copy in b_shares:
            copy.wait_recv()
        for copy in loads[6:]:
            copy.wait()
        for s in range(n_fs):
            wide[s * rows : (s + 1) * rows, :] = shares[s].astype(f32)
        for i, (first, second, first_new, second_new) in enumerate(
            (
                (value_moment, value_second, value_moment_new, value_second_new),
                (output_moment, output_second, output_moment_new, output_second_new),
            )
        ):
            span = slice(starts[i], starts[i] + cols[i])

            def body(r, gathered, first=first, second=second, first_new=first_new,
                     second_new=second_new, span=span, i=i):
                at = pl.ds(pl.multiple_of(r * block, block), block)
                projected = wide[at, span]
                m = BETA_ONE * first[at, :] + (1.0 - BETA_ONE) * projected
                v = BETA_TWO * second[at, :] + (1.0 - BETA_TWO) * projected * projected
                norm = m / (jnp.sqrt(v) + EPSILON)
                first_new[at, :] = m
                second_new[at, :] = v
                wide[at, span] = norm
                square = norm * norm
                square = square[:8] + square[8:]
                for c in range(cols[i] // 128):
                    gathered += square[:, c * 128 : (c + 1) * 128]
                return gathered

            squares[i] = lax.fori_loop(
                0, rank // block, body, jnp.zeros((8, 128), f32)
            )
        for copy in square_copies:
            copy.start()

    def steps():
        for copy in square_copies:
            copy.wait()
        for i, (factor, master, step, new) in enumerate(
            (
                (value_factor, value_master, value_step, value_new),
                (output_factor, output_master, output_step, output_new),
            )
        ):
            gathered = squares[i]
            for k in range(n_tp - 1):
                gathered += near_squares[k, i]
            gathered = jnp.sum(jnp.sum(gathered, axis=1, keepdims=True), axis=0, keepdims=True)
            scale = lax.rsqrt(gathered / (rank * cols[i] * n_tp) + FLOOR)
            span = slice(starts[i], starts[i] + cols[i])

            def body(r, carry, span=span, scale=scale, width=cols[i]):
                at = pl.ds(pl.multiple_of(r * block, block), block)
                scaled = wide[at, span] * jnp.broadcast_to(scale, (block, width))
                rounded = scaled.astype(bf16)
                high[at, span] = rounded
                low[at, span] = (scaled - rounded.astype(f32)).astype(bf16)
                return carry

            lax.fori_loop(0, rank // block, body, 0)
            height = master.shape[0]
            here = factor[pl.ds(pl.multiple_of(me * height, height), height), :]
            tile = 512 if cols[i] % 512 == 0 else cols[i]
            for c in range(cols[i] // tile):
                at = slice(c * tile, (c + 1) * tile)
                inner = slice(starts[i] + c * tile, starts[i] + (c + 1) * tile)
                moved = jnp.dot(here, high[:, inner], preferred_element_type=f32) + jnp.dot(
                    here, low[:, inner], preferred_element_type=f32
                )
                step[:, at] = moved
                new[:, at] = master[:, at] - STEP_RATE * moved

    def copies(level, i):
        source_z = level_z(n_z, here_z, level)
        factor = (value_factor, output_factor)[i]
        renew(source_z, factor, high, starts[i], alls[i], alls[i], source_z * PLANE)

    work = [
        (0.5, products),
        (stages[0], second_sum),
        (stages[1], third_sum),
        (stages[2], last_sum),
        (stages[3], share_a),
        (stages[4], share_b),
        (stages[5], moments),
        (stages[5] + 0.5, steps),
    ]
    free = stages[5] + 0.6
    ready = []
    for level in range(n_z - 1):
        for i in range(2):
            when = 0.0
            for k in range(len(roles)):
                offset = levels_of(n_z, k)[level]
                for at, _, kind, _, item in roles[k][0]:
                    if item[0] == offset and classes[item[3]][0] == i:
                        when = max(when, at)
            ready.append((when, len(ready), level, i))
    for when, _, level, i in sorted(ready):
        free = max(free + 0.45, when + 0.01)
        work.append((free, functools.partial(copies, level, i)))

    before = -1.0
    for when, action in sorted(work, key=lambda x: x[0]):
        for k in range(len(roles)):
            run_events(k, before, when)
        action()
        before = when
    for k in range(len(roles)):
        run_events(k, before, float("inf"))
    for copy in pending:
        copy.wait_send()


def per_device(
    n_fs,
    n_tp,
    normed_input,
    value_cotangent,
    mixer_output,
    output_cotangent,
    value_factor,
    output_factor,
    value_master,
    value_moment,
    value_second,
    output_master,
    output_moment,
    output_second,
):
    f32, bf16 = jnp.float32, jnp.bfloat16
    rank = value_factor.shape[1]
    rows = rank // n_fs
    n_z = n_fs // PLANE
    tokens, value_cols = value_cotangent.shape
    output_cols = output_cotangent.shape[1]
    both = value_cols + output_cols
    others = max(n_tp - 1, 1)
    dma = pltpu.SemaphoreType.DMA
    stacks = []
    for master in (value_master, output_master):
        count = pieces_of(*master.shape)
        stacks.append((n_fs, count, master.shape[0] // count, master.shape[1]))
    n_pieces = stacks[0][1] + stacks[1][1]
    streamed = (
        normed_input,
        mixer_output,
        value_cotangent,
        output_cotangent,
        value_factor,
        output_factor,
        value_moment,
        value_second,
        output_moment,
        output_second,
        value_master,
        output_master,
    )
    outs = []
    for master, moment, stack in (
        (value_master, value_moment, stacks[0]),
        (output_master, output_moment, stacks[1]),
    ):
        outs += [
            (master.shape, f32),
            (master.shape, f32),
            (stack, bf16),
            (moment.shape, f32),
            (moment.shape, f32),
        ]
    outs += [(value_factor.shape, bf16), (output_factor.shape, bf16), ((rank, both), bf16)]
    room = (62 << 20) - sum(math.prod(x) * jnp.dtype(t).itemsize for x, t in outs)
    held = [x for x in streamed if x is not value_factor and x is not output_factor]
    results = pl.pallas_call(
        functools.partial(step_kernel, n_fs, n_tp),
        out_shape=tuple(pltpu.VMEM(*x) for x in outs),
        in_specs=[pl.BlockSpec(memory_space=pltpu.HBM)] * len(streamed),
        out_specs=(pl.BlockSpec(memory_space=pltpu.VMEM),) * len(outs),
        scratch_shapes=[pltpu.VMEM(x.shape, x.dtype) for x in held]
        + [
            dma((10,)),
            dma((n_pieces,)),
            pltpu.VMEM((tokens, rank), bf16),
            pltpu.VMEM((tokens, rank), bf16),
            pltpu.VMEM((others, tokens, rank), bf16),
            pltpu.VMEM((others, tokens, rank), bf16),
            pltpu.VMEM((2, 8, 128), f32),
            pltpu.VMEM((others, 2, 8, 128), f32),
            pltpu.VMEM((n_fs, rows, both), f32),
            pltpu.VMEM((n_fs, rows, both), bf16),
            pltpu.VMEM((n_fs // 2, rows, both), bf16),
            pltpu.VMEM((n_z, rows, both), bf16),
            pltpu.VMEM((n_z, rows, both), bf16),
            pltpu.VMEM((n_z, rows, both), f32),
            pltpu.VMEM((n_z, rows, both), bf16),
            pltpu.VMEM((n_z, rows, both), bf16),
            pltpu.VMEM((n_fs, rows, both), bf16),
            pltpu.VMEM((rank, both), f32),
            pltpu.VMEM((rank, both), bf16),
            dma((others, 3)),
            dma((others, 3)),
            dma((n_z + 1,)),
            dma((n_z + 1,)),
            dma((n_z + 2,)),
            dma((n_z + 2,)),
            dma((4, n_fs, n_pieces)),
            dma((n_fs, n_pieces)),
        ],
        compiler_params=pltpu.CompilerParams(
            collective_id=0, has_side_effects=True, vmem_limit_bytes=room
        ),
    )(*streamed)
    return store(n_fs, results)


def store_kernel(n_fs, *refs):
    results, (value_factor, output_factor, high) = refs[:10], refs[10:13]
    outs, last, sem = refs[13:23], refs[23:25], refs[25]
    n_z = n_fs // PLANE
    here_z = lax.axis_index("fs") // PLANE
    copies = []

    def begin(src, dst):
        copy = pltpu.make_async_copy(src, dst, sem.at[len(copies)])
        copy.start()
        copies.append(copy)

    for level in range(n_z - 1):
        at = pl.ds(level_z(n_z, here_z, level) * PLANE, PLANE)
        for i in (2, 7):
            begin(results[i].at[at], outs[i].at[at])
    for i in range(10):
        if i % 5 != 2:
            begin(results[i], outs[i])
    far = level_z(n_z, here_z, n_z - 1)
    start = 0
    for i, factor in enumerate((value_factor, output_factor)):
        old = results[2 + 5 * i]
        renew(far, factor, high, start, old, last[i], 0)
        start += old.shape[3]
        begin(last[i], outs[2 + 5 * i].at[pl.ds(far * PLANE, PLANE)])
    for copy in copies:
        copy.wait()


def store(n_fs, arrays):
    outs = [jax.ShapeDtypeStruct(x.shape, x.dtype) for x in arrays[:10]]
    results = list(
        pl.pallas_call(
            functools.partial(store_kernel, n_fs),
            out_shape=tuple(outs),
            in_specs=[pl.BlockSpec(memory_space=pltpu.VMEM)] * len(arrays),
            out_specs=(pl.BlockSpec(memory_space=pltpu.HBM),) * len(outs),
            scratch_shapes=[
                pltpu.VMEM((PLANE,) + arrays[i].shape[1:], jnp.bfloat16) for i in (2, 7)
            ]
            + [pltpu.SemaphoreType.DMA((2 * (n_fs // PLANE) + 8,))],
            compiler_params=pltpu.CompilerParams(vmem_limit_bytes=6 << 20),
        )(*arrays)
    )
    for i in (2, 7):
        results[i] = results[i].reshape(-1, results[i].shape[3])
    return tuple(results)


def solution(mesh):
    return jax.shard_map(
        functools.partial(per_device, mesh.shape["fs"], mesh.shape["tp"]),
        mesh=mesh,
        in_specs=(
            P("fs", "tp"),
            P("fs", "tp"),
            P("fs", "tp"),
            P("fs", "tp"),
            P(),
            P(),
            P("fs", "tp"),
            P(None, "tp"),
            P(None, "tp"),
            P("fs", "tp"),
            P(None, "tp"),
            P(None, "tp"),
        ),
        out_specs=(
            P("fs", "tp"),
            P("fs", "tp"),
            P(None, "tp"),
            P(None, "tp"),
            P(None, "tp"),
            P("fs", "tp"),
            P("fs", "tp"),
            P(None, "tp"),
            P(None, "tp"),
            P(None, "tp"),
        ),
        check_vma=False,
    )
```

```python
import collections
import functools
import math

import jax
import jax.numpy as jnp
from jax import lax
from jax.experimental import pallas as pl
from jax.experimental.pallas import tpu as pltpu
from jax.sharding import PartitionSpec as P

BETA_ONE = 0.8
BETA_TWO = 0.9
EPSILON = 1e-08
STEP_RATE = 0.005
FLOOR = 0.25

MESH = pl.DeviceIdType.MESH
A, B, UP, DOWN = range(4)
PLANE = 4
GRAIN = 1
LATENCY = 6
LEAD = 3.0
FLIGHT = 1.75


def pieces_of(rows, cols):
    count = max(1, min(4 * GRAIN, rows * cols * 2 * GRAIN // 131072))
    while rows % (16 * count):
        count -= 1
    return count


def classes_of(counts):
    out = []
    for array, count in enumerate(counts):
        for p in range(count):
            plane_first = count % 4 == 0 and p % 4 == 3
            out.append((array, p, plane_first, A if (p + array) % 2 == 0 else B))
    return out


def onward(n_z, classes, z, item, via):
    _, fa, fb, p = item
    _, _, plane_first, order = classes[p]
    up = [UP] if z < n_z - 1 else []
    down = [DOWN] if z > 0 else []
    if via is None:
        return [A, B] + up + down
    if via in (UP, DOWN):
        return (up if via == UP else down) + ([] if plane_first else [A, B])
    links = []
    if (fa, fb) == (1, 0) and order == A:
        links.append(B)
    if (fa, fb) == (0, 1) and order == B:
        links.append(A)
    return links + (up + down if plane_first else [])


def hops_left(n_z, classes, z, item, link):
    _, fa, fb, p = item
    _, _, plane_first, order = classes[p]
    if link in (UP, DOWN):
        return (n_z - 2 - z if link == UP else z - 1) + (0 if plane_first else 2)
    turn = 1 if link == order and (fa, fb) == (0, 0) else 0
    return turn + (max(n_z - 1 - z, z) if plane_first else 0)


def plan(n_z, classes, reserved):
    pool = collections.defaultdict(list)
    arriving = collections.defaultdict(list)
    sends = {z: [] for z in range(n_z)}
    takes = {z: [] for z in range(n_z)}
    busy = collections.defaultdict(int)
    for z in range(n_z):
        for p in range(len(classes)):
            item = (z, 0, 0, p)
            for link in onward(n_z, classes, z, item, None):
                pool[z, link].append((0, item))
    missing = n_z * (n_z * PLANE - 1) * len(classes)
    tick = 0
    while missing:
        for z, item, via in arriving.pop(tick, ()):
            for link in onward(n_z, classes, z, item, via):
                pool[z, link].append((tick, item))
        for z in range(n_z):
            toward = 1 if 2 * z < n_z else -1
            for link in range(4):
                held = [
                    n * GRAIN
                    for start, way, n in reserved
                    if way == link and start * GRAIN == tick
                ]
                if held:
                    busy[z, link] = tick + held[0]
                waiting = pool[z, link]
                if busy[z, link] > tick or not waiting:
                    continue
                best = max(
                    waiting,
                    key=lambda x: (
                        hops_left(n_z, classes, z, x[1], link),
                        -abs(x[1][0] - z),
                        (x[1][0] - z) * toward,
                        -x[1][3],
                        -x[0],
                        -x[1][1],
                        -x[1][2],
                    ),
                )
                waiting.remove(best)
                item = best[1]
                source, fa, fb, p = item
                sends[z].append((tick, link, item))
                if link == A:
                    there, got = z, (source, 1 - fa, fb, p)
                elif link == B:
                    there, got = z, (source, fa, 1 - fb, p)
                else:
                    there, got = z + (1 if link == UP else -1), item
                takes[there].append((tick, link, got))
                arriving[tick + LATENCY * GRAIN].append((there, got, link))
                busy[z, link] = tick + 1
                missing -= 1
        tick += 1
    return sends, takes


def mirrored(n_z, events):
    swap = {A: A, B: B, UP: DOWN, DOWN: UP}
    return sorted(
        (tick, swap[link], (n_z - 1 - s, fa, fb, p)) for tick, link, (s, fa, fb, p) in events
    )


def roles_of(n_z, sends, takes):
    pairs = n_z % 2 == 0 and all(
        sorted(x[z]) == mirrored(n_z, x[n_z - 1 - z])
        for x in (sends, takes)
        for z in range(n_z // 2)
    )
    roles = []
    for z in range(n_z // 2 if pairs else n_z):
        events = []
        done = {}
        for tick, link, (source, fa, fb, p) in sorted(takes[z]):
            item = (source - z, fa, fb, p)
            done[item] = tick / GRAIN + FLIGHT
            events.append((done[item], 0, "take", link, item))
        last = collections.defaultdict(float)
        for tick, link, (source, fa, fb, p) in sorted(sends[z]):
            item = (source - z, fa, fb, p)
            at = tick / GRAIN
            when = max(at - LEAD, done.get(item, 0.0), last[link])
            if item not in done and at <= 4:
                when = 0.0
            last[link] = when
            events.append((when, 1, "send", link, item))
            events.append((max(at + 3.0, when + 2.0), 2, "sent", link, item))
        roles.append((sorted(events, key=lambda e: e[:2]), done))
    return pairs, roles


def levels_of(n_z, z):
    near, toward = (z, 1) if 2 * z < n_z else (n_z - 1 - z, -1)
    out = []
    for level in range(n_z):
        step = (level + 1) // 2 if level % 2 else -(level // 2)
        out.append(toward * (step if level <= 2 * near else level - near))
    return out


def level_z(n_z, here_z, level):
    near = jnp.where(2 * here_z < n_z, here_z, n_z - 1 - here_z)
    toward = jnp.where(2 * here_z < n_z, 1, -1)
    step = (level + 1) // 2 if level % 2 else -(level // 2)
    return here_z + toward * jnp.where(level <= 2 * near, step, level - near)


def renew(source_z, factor, high, start, old, out, first):
    _, count, height, cols = old.shape
    tall = count * height
    tile = 512 if cols % 512 == 0 else cols

    def body(c, carry):
        source = source_z * PLANE + c
        here = factor[pl.ds(pl.multiple_of(source * tall, tall), tall), :]
        for t in range(cols // tile):
            at = slice(t * tile, (t + 1) * tile)
            inner = slice(start + t * tile, start + (t + 1) * tile)
            moved = jnp.dot(here, high[:, inner], preferred_element_type=jnp.float32)
            for p in range(count):
                fresh = (
                    old[source, p, :, at].astype(jnp.float32)
                    - STEP_RATE * moved[p * height : (p + 1) * height]
                )
                out[first + c, p, :, at] = fresh.astype(jnp.bfloat16)
        return carry

    lax.fori_loop(0, PLANE, body, 0)


def step_kernel(
    n_fs,
    n_tp,
    normed_hbm,
    mixer_hbm,
    value_cot_hbm,
    output_cot_hbm,
    value_factor_hbm,
    output_factor_hbm,
    value_moment_hbm,
    value_second_hbm,
    output_moment_hbm,
    output_second_hbm,
    value_master_hbm,
    output_master_hbm,
    value_step,
    value_new,
    value_all,
    value_moment_new,
    value_second_new,
    output_step,
    output_new,
    output_all,
    output_moment_new,
    output_second_new,
    value_factor,
    output_factor,
    high,
    normed,
    mixer,
    value_cot,
    output_cot,
    value_moment,
    value_second,
    output_moment,
    output_second,
    value_master,
    output_master,
    load_sem,
    master_sem,
    input_ref,
    mixer_ref,
    near_in,
    near_mix,
    squares,
    near_squares,
    total,
    part,
    a_recv,
    b_part,
    b_recv,
    quarter,
    z_part,
    z_recv,
    shares,
    wide,
    low,
    near_send,
    near_recv,
    sum_send,
    sum_recv,
    share_send,
    share_recv,
    gather_send,
    gather_recv,
):
    f32, bf16 = jnp.float32, jnp.bfloat16
    me = lax.axis_index("fs")
    column = lax.axis_index("tp")
    n_z = n_fs // PLANE
    half = n_fs // 2
    here_a = lax.rem(me, 2)
    here_b = lax.rem(me // 2, 2)
    here_z = me // PLANE
    alls = (value_all, output_all)
    rows = total.shape[1]
    cols = (value_cot.shape[1], output_cot.shape[1])
    starts = (0, cols[0])
    classes = classes_of([x.shape[1] for x in alls])
    fine = len(classes) == 8 * GRAIN

    if fine:
        reserved = (
            (4, A, 3),
            (10, B, 2),
            (15, UP, 1),
            (15, DOWN, 1),
            (20, UP, 1),
            (20, DOWN, 1),
            (25, A, 2),
            (30, B, 3),
        )
        stages = (7.8, 12.8, 17.8, 22.8, 27.8, 33.8)
    else:
        reserved = ()
        stages = tuple(7.8 + 4 * i for i in range(6))
    sends, takes = plan(n_z, classes, reserved)
    pairs, roles = roles_of(n_z, sends, takes)
    if pairs:
        toward = jnp.where(2 * here_z < n_z, 1, -1)
        role = jnp.where(2 * here_z < n_z, here_z, n_z - 1 - here_z)
    else:
        toward = 1
        role = here_z

    across_a = me + 1 - 2 * here_a
    across_b = me + 2 - 4 * here_b
    targets = {
        A: across_a,
        B: across_b,
        UP: me + toward * PLANE,
        DOWN: me - toward * PLANE,
    }
    places = {
        (fa, fb): (1 - here_b if fb else here_b) * 2 + (1 - here_a if fa else here_a)
        for fa in range(2)
        for fb in range(2)
    }

    def z_mate(k):
        return lax.rem(here_z + k, n_z) * PLANE + lax.rem(me, PLANE)

    masters = []
    for array, p, _, _ in classes:
        hbm, master = ((value_master_hbm, value_master), (output_master_hbm, output_master))[array]
        height = alls[array].shape[2]
        at = pl.ds(p * height, height)
        masters.append(
            pltpu.make_async_copy(hbm.at[at], master.at[at], master_sem.at[len(masters)])
        )
    loads = [
        pltpu.make_async_copy(src, dst, load_sem.at[i])
        for i, (src, dst) in enumerate(
            (
                (mixer_hbm, mixer),
                (output_factor_hbm, output_factor),
                (normed_hbm, normed),
                (value_factor_hbm, value_factor),
                (value_cot_hbm, value_cot),
                (output_cot_hbm, output_cot),
                (value_moment_hbm, value_moment),
                (value_second_hbm, value_second),
                (output_moment_hbm, output_moment),
                (output_second_hbm, output_second),
            )
        )
    ]

    opening = [[] for _ in classes]
    for k, (events, _) in enumerate(roles):
        for when, _, kind, link, item in events:
            if kind == "send" and when == 0.0:
                opening[item[3]].append((k, link, item))
    queue = sorted(
        range(len(classes)),
        key=lambda p: min(
            [t for z in sends for t, _, item in sends[z] if item == (z, 0, 0, p)]
        ),
    )
    for p in queue:
        masters[p].start()

    barrier = pltpu.get_barrier_semaphore()
    for there in [across_a, across_b] + [z_mate(k) for k in range(1, n_z)]:
        pl.semaphore_signal(barrier, inc=1, device_id={"fs": there}, device_id_type=MESH)
    for k in range(1, n_tp):
        pl.semaphore_signal(
            barrier,
            inc=1,
            device_id={"tp": lax.rem(column + k, n_tp)},
            device_id_type=MESH,
        )

    def piece_copy(link, item):
        offset, fa, fb, p = item
        source = (here_z + toward * offset) * PLANE + places[fa, fb]
        array, piece, _, _ = classes[p]
        there = alls[array].at[source, piece]
        return pltpu.make_async_remote_copy(
            src_ref=there,
            dst_ref=there,
            send_sem=gather_send.at[link, source, p],
            recv_sem=gather_recv.at[source, p],
            device_id={"fs": targets[link]},
            device_id_type=MESH,
        )

    def open_piece(p):
        for k in range(len(roles)):
            out = [x for x in opening[p] if x[0] == k]
            if out:

                @pl.when(role == k)
                def _(out=out):
                    for _, link, item in out:
                        piece_copy(link, item).start()

    for n, p in enumerate(queue):
        masters[p].wait()
        array, piece, _, _ = classes[p]
        height = alls[array].shape[2]
        master = (value_master, output_master)[array]
        alls[array][me, piece] = master[piece * height : (piece + 1) * height, :].astype(bf16)
        if n == len(queue) - 1:
            for copy in loads:
                copy.start()
        if n == 0:
            pl.semaphore_wait(barrier, 2 + (n_z - 1) + (n_tp - 1))
        else:
            open_piece(queue[n - 1])
    open_piece(queue[-1])

    def run_events(k, first, last):
        events = [
            e for e in roles[k][0] if first <= e[0] < last and (e[2] != "send" or e[0] > 0.0)
        ]
        if not events:
            return

        @pl.when(role == k)
        def _():
            for _, _, kind, link, item in events:
                copy = piece_copy(link, item)
                if kind == "take":
                    copy.wait_recv()
                elif kind == "send":
                    copy.start()
                else:
                    copy.wait_send()

    def message(src, dst, there, sems, index):
        send, recv = sems
        return pltpu.make_async_remote_copy(
            src_ref=src,
            dst_ref=dst,
            send_sem=send.at[index],
            recv_sem=recv.at[index],
            device_id={"fs": there},
            device_id_type=MESH,
        )

    sums = (sum_send, sum_recv)
    shared = (share_send, share_recv)
    pending = []

    def start(copies):
        for copy in copies:
            copy.start()
        pending.extend(copies)
        return copies

    a_sum = message(part.at[pl.ds((1 - here_a) * half, half)], a_recv, across_a, sums, 0)
    b_sum = message(b_part, b_recv, across_b, sums, n_z)
    owners = n_z // 2 if n_z % 4 == 0 else n_z
    edge = (n_z - owners) // 2
    depth = n_z // owners
    mine = here_a * half + here_b * n_z
    is_owner = jnp.logical_and(here_z >= edge, here_z < edge + owners)

    def z_sum(j, k):
        return message(
            z_part.at[pl.ds(j * depth, depth)],
            z_recv.at[k],
            (edge + j) * PLANE + lax.rem(me, PLANE),
            sums,
            k,
        )

    def z_share(j, k):
        at = shares.at[pl.ds(mine + j * depth, depth)]
        return message(at, at, lax.rem(edge + j + k, n_z) * PLANE + lax.rem(me, PLANE), shared, k)
    ours = shares.at[pl.ds(mine, n_z)]
    other = shares.at[pl.ds((1 - here_a) * half + here_b * n_z, n_z)]
    a_share = message(ours, ours, across_a, shared, 0)
    b_shares = [
        message(ours, ours, across_b, shared, n_z),
        message(other, other, across_b, shared, n_z + 1),
    ]

    def products():
        near = []
        for i, (tokens, factor, own, dst) in enumerate(
            (
                (mixer, output_factor, mixer_ref, near_mix),
                (normed, value_factor, input_ref, near_in),
            )
        ):
            loads[2 * i].wait()
            loads[2 * i + 1].wait()
            depth = tokens.shape[1]
            rows_here = factor[pl.ds(pl.multiple_of(column * depth, depth), depth), :]
            own[...] = jnp.dot(
                tokens[...], rows_here, preferred_element_type=f32
            ).astype(bf16)
            for k in range(1, n_tp):
                copy = pltpu.make_async_remote_copy(
                    src_ref=own,
                    dst_ref=dst.at[k - 1],
                    send_sem=near_send.at[k - 1, i],
                    recv_sem=near_recv.at[k - 1, i],
                    device_id={"tp": lax.rem(column + k, n_tp)},
                    device_id_type=MESH,
                )
                copy.start()
                near.append(copy)
        for copy in near:
            copy.wait()
        input_total = input_ref[...].astype(f32)
        mixer_total = mixer_ref[...].astype(f32)
        for k in range(n_tp - 1):
            input_total += near_in[k].astype(f32)
            mixer_total += near_mix[k].astype(f32)
        for copy in loads[4:6]:
            copy.wait()
        across = (((0,), (0,)), ((), ()))
        for i, (left, right) in enumerate(
            (
                (input_total.astype(bf16), value_cot),
                (mixer_total.astype(bf16), output_cot),
            )
        ):
            tile = 512 if cols[i] % 512 == 0 else cols[i]
            for c in range(cols[i] // tile):
                product = lax.dot_general(
                    left,
                    right[:, c * tile : (c + 1) * tile],
                    across,
                    preferred_element_type=f32,
                )
                at = slice(starts[i] + c * tile, starts[i] + (c + 1) * tile)
                for s in range(n_fs):
                    block = product[s * rows : (s + 1) * rows]
                    total[s, :, at] = block
                    part[s, :, at] = block.astype(bf16)
        start([a_sum])

    def second_sum():
        a_sum.wait_recv()
        away = (1 - here_b) * n_z
        b_part[...] = (
            total[pl.ds(here_a * half + away, n_z)] + a_recv[pl.ds(away, n_z)].astype(f32)
        ).astype(bf16)
        start([b_sum])
        quarter[...] = total[pl.ds(mine, n_z)] + a_recv[pl.ds(here_b * n_z, n_z)].astype(f32)

    def third_sum():
        b_sum.wait_recv()
        quarter[...] += b_recv[...].astype(f32)
        z_part[...] = quarter[...].astype(bf16)
        for j in range(owners):

            @pl.when(here_z != edge + j)
            def _(j=j):
                z_sum(j, lax.rem(edge + j - here_z + n_z, n_z)).start()

    def last_sum():
        @pl.when(is_owner)
        def _():
            j = here_z - edge
            done = quarter[pl.ds(j * depth, depth)]
            for k in range(1, n_z):
                z_sum(j, k).wait_recv()
                done += z_recv[k].astype(f32)
            shares[pl.ds(mine + j * depth, depth)] = done.astype(bf16)
            for k in range(1, n_z):
                z_share(j, k).start()

    def share_a():
        for j in range(owners):

            @pl.when(here_z != edge + j)
            def _(j=j):
                z_share(j, lax.rem(here_z - edge - j + n_z, n_z)).wait_recv()

        start([a_share])

    def settle():
        for copy in pending:
            copy.wait_send()
        for j in range(owners):

            @pl.when(here_z != edge + j)
            def _(j=j):
                z_sum(j, lax.rem(edge + j - here_z + n_z, n_z)).wait_send()

        @pl.when(is_owner)
        def _():
            for k in range(1, n_z):
                z_share(here_z - edge, k).wait_send()

    def share_b():
        a_share.wait_recv()
        start(b_shares)

    square_copies = [
        pltpu.make_async_remote_copy(
            src_ref=squares,
            dst_ref=near_squares.at[k - 1],
            send_sem=near_send.at[k - 1, 2],
            recv_sem=near_recv.at[k - 1, 2],
            device_id={"tp": lax.rem(column + k, n_tp)},
            device_id_type=MESH,
        )
        for k in range(1, n_tp)
    ]
    rank = value_factor.shape[1]
    block = 16

    def moments():
        for copy in b_shares:
            copy.wait_recv()
        for copy in loads[6:]:
            copy.wait()
        for s in range(n_fs):
            wide[s * rows : (s + 1) * rows, :] = shares[s].astype(f32)
        for i, (first, second, first_new, second_new) in enumerate(
            (
                (value_moment, value_second, value_moment_new, value_second_new),
                (output_moment, output_second, output_moment_new, output_second_new),
            )
        ):
            span = slice(starts[i], starts[i] + cols[i])

            def body(r, gathered, first=first, second=second, first_new=first_new,
                     second_new=second_new, span=span, i=i):
                at = pl.ds(pl.multiple_of(r * block, block), block)
                projected = wide[at, span]
                m = BETA_ONE * first[at, :] + (1.0 - BETA_ONE) * projected
                v = BETA_TWO * second[at, :] + (1.0 - BETA_TWO) * projected * projected
                norm = m / (jnp.sqrt(v) + EPSILON)
                first_new[at, :] = m
                second_new[at, :] = v
                wide[at, span] = norm
                square = norm * norm
                square = square[:8] + square[8:]
                for c in range(cols[i] // 128):
                    gathered += square[:, c * 128 : (c + 1) * 128]
                return gathered

            squares[i] = lax.fori_loop(
                0, rank // block, body, jnp.zeros((8, 128), f32)
            )
        for copy in square_copies:
            copy.start()

    def steps():
        for copy in square_copies:
            copy.wait()
        for i, (factor, master, step, new) in enumerate(
            (
                (value_factor, value_master, value_step, value_new),
                (output_factor, output_master, output_step, output_new),
            )
        ):
            gathered = squares[i]
            for k in range(n_tp - 1):
                gathered += near_squares[k, i]
            gathered = jnp.sum(jnp.sum(gathered, axis=1, keepdims=True), axis=0, keepdims=True)
            scale = lax.rsqrt(gathered / (rank * cols[i] * n_tp) + FLOOR)
            span = slice(starts[i], starts[i] + cols[i])

            def body(r, carry, span=span, scale=scale, width=cols[i]):
                at = pl.ds(pl.multiple_of(r * block, block), block)
                scaled = wide[at, span] * jnp.broadcast_to(scale, (block, width))
                rounded = scaled.astype(bf16)
                high[at, span] = rounded
                low[at, span] = (scaled - rounded.astype(f32)).astype(bf16)
                return carry

            lax.fori_loop(0, rank // block, body, 0)
            height = master.shape[0]
            here = factor[pl.ds(pl.multiple_of(me * height, height), height), :]
            tile = 512 if cols[i] % 512 == 0 else cols[i]
            for c in range(cols[i] // tile):
                at = slice(c * tile, (c + 1) * tile)
                inner = slice(starts[i] + c * tile, starts[i] + (c + 1) * tile)
                moved = jnp.dot(here, high[:, inner], preferred_element_type=f32) + jnp.dot(
                    here, low[:, inner], preferred_element_type=f32
                )
                step[:, at] = moved
                new[:, at] = master[:, at] - STEP_RATE * moved

    def copies(level, i):
        source_z = level_z(n_z, here_z, level)
        factor = (value_factor, output_factor)[i]
        renew(source_z, factor, high, starts[i], alls[i], alls[i], source_z * PLANE)

    work = [
        (0.5, products),
        (stages[0], second_sum),
        (stages[1], third_sum),
        (stages[2], last_sum),
        (stages[3], share_a),
        (stages[4], share_b),
        (stages[5], moments),
        (stages[5] + 0.5, steps),
    ]
    free = stages[5] + 0.6
    ready = []
    for level in range(n_z - 1):
        for i in range(2):
            when = 0.0
            for k in range(len(roles)):
                offset = levels_of(n_z, k)[level]
                for at, _, kind, _, item in roles[k][0]:
                    if item[0] == offset and classes[item[3]][0] == i:
                        when = max(when, at)
            ready.append((when, len(ready), level, i))
    for when, _, level, i in sorted(ready):
        free = max(free + 0.45, when + 0.01)
        work.append((free, functools.partial(copies, level, i)))

    before = -1.0
    for when, action in sorted(work, key=lambda x: x[0]):
        for k in range(len(roles)):
            run_events(k, before, when)
        action()
        before = when
    for k in range(len(roles)):
        run_events(k, before, float("inf"))
    settle()


def per_device(
    n_fs,
    n_tp,
    normed_input,
    value_cotangent,
    mixer_output,
    output_cotangent,
    value_factor,
    output_factor,
    value_master,
    value_moment,
    value_second,
    output_master,
    output_moment,
    output_second,
):
    f32, bf16 = jnp.float32, jnp.bfloat16
    rank = value_factor.shape[1]
    rows = rank // n_fs
    n_z = n_fs // PLANE
    tokens, value_cols = value_cotangent.shape
    output_cols = output_cotangent.shape[1]
    both = value_cols + output_cols
    others = max(n_tp - 1, 1)
    dma = pltpu.SemaphoreType.DMA
    stacks = []
    for master in (value_master, output_master):
        count = pieces_of(*master.shape)
        stacks.append((n_fs, count, master.shape[0] // count, master.shape[1]))
    n_pieces = stacks[0][1] + stacks[1][1]
    streamed = (
        normed_input,
        mixer_output,
        value_cotangent,
        output_cotangent,
        value_factor,
        output_factor,
        value_moment,
        value_second,
        output_moment,
        output_second,
        value_master,
        output_master,
    )
    outs = []
    for master, moment, stack in (
        (value_master, value_moment, stacks[0]),
        (output_master, output_moment, stacks[1]),
    ):
        outs += [
            (master.shape, f32),
            (master.shape, f32),
            (stack, bf16),
            (moment.shape, f32),
            (moment.shape, f32),
        ]
    outs += [(value_factor.shape, bf16), (output_factor.shape, bf16), ((rank, both), bf16)]
    room = (62 << 20) - sum(math.prod(x) * jnp.dtype(t).itemsize for x, t in outs)
    held = [x for x in streamed if x is not value_factor and x is not output_factor]
    results = pl.pallas_call(
        functools.partial(step_kernel, n_fs, n_tp),
        out_shape=tuple(pltpu.VMEM(*x) for x in outs),
        in_specs=[pl.BlockSpec(memory_space=pltpu.HBM)] * len(streamed),
        out_specs=(pl.BlockSpec(memory_space=pltpu.VMEM),) * len(outs),
        scratch_shapes=[pltpu.VMEM(x.shape, x.dtype) for x in held]
        + [
            dma((10,)),
            dma((n_pieces,)),
            pltpu.VMEM((tokens, rank), bf16),
            pltpu.VMEM((tokens, rank), bf16),
            pltpu.VMEM((others, tokens, rank), bf16),
            pltpu.VMEM((others, tokens, rank), bf16),
            pltpu.VMEM((2, 8, 128), f32),
            pltpu.VMEM((others, 2, 8, 128), f32),
            pltpu.VMEM((n_fs, rows, both), f32),
            pltpu.VMEM((n_fs, rows, both), bf16),
            pltpu.VMEM((n_fs // 2, rows, both), bf16),
            pltpu.VMEM((n_z, rows, both), bf16),
            pltpu.VMEM((n_z, rows, both), bf16),
            pltpu.VMEM((n_z, rows, both), f32),
            pltpu.VMEM((n_z, rows, both), bf16),
            pltpu.VMEM((n_z, 2 if n_z % 4 == 0 else 1, rows, both), bf16),
            pltpu.VMEM((n_fs, rows, both), bf16),
            pltpu.VMEM((rank, both), f32),
            pltpu.VMEM((rank, both), bf16),
            dma((others, 3)),
            dma((others, 3)),
            dma((n_z + 1,)),
            dma((n_z + 1,)),
            dma((n_z + 2,)),
            dma((n_z + 2,)),
            dma((4, n_fs, n_pieces)),
            dma((n_fs, n_pieces)),
        ],
        compiler_params=pltpu.CompilerParams(
            collective_id=0, has_side_effects=True, vmem_limit_bytes=room
        ),
    )(*streamed)
    return store(n_fs, results)


def store_kernel(n_fs, *refs):
    results, (value_factor, output_factor, high) = refs[:10], refs[10:13]
    outs, last, sem = refs[13:23], refs[23:25], refs[25]
    n_z = n_fs // PLANE
    here_z = lax.axis_index("fs") // PLANE
    copies = []

    def begin(src, dst):
        copy = pltpu.make_async_copy(src, dst, sem.at[len(copies)])
        copy.start()
        copies.append(copy)

    for level in range(n_z - 1):
        at = pl.ds(level_z(n_z, here_z, level) * PLANE, PLANE)
        for i in (2, 7):
            begin(results[i].at[at], outs[i].at[at])
    for i in range(10):
        if i % 5 != 2:
            begin(results[i], outs[i])
    far = level_z(n_z, here_z, n_z - 1)
    start = 0
    for i, factor in enumerate((value_factor, output_factor)):
        old = results[2 + 5 * i]
        renew(far, factor, high, start, old, last[i], 0)
        start += old.shape[3]
        begin(last[i], outs[2 + 5 * i].at[pl.ds(far * PLANE, PLANE)])
    for copy in copies:
        copy.wait()


def store(n_fs, arrays):
    outs = [jax.ShapeDtypeStruct(x.shape, x.dtype) for x in arrays[:10]]
    results = list(
        pl.pallas_call(
            functools.partial(store_kernel, n_fs),
            out_shape=tuple(outs),
            in_specs=[pl.BlockSpec(memory_space=pltpu.VMEM)] * len(arrays),
            out_specs=(pl.BlockSpec(memory_space=pltpu.HBM),) * len(outs),
            scratch_shapes=[
                pltpu.VMEM((PLANE,) + arrays[i].shape[1:], jnp.bfloat16) for i in (2, 7)
            ]
            + [pltpu.SemaphoreType.DMA((2 * (n_fs // PLANE) + 8,))],
            compiler_params=pltpu.CompilerParams(vmem_limit_bytes=6 << 20),
        )(*arrays)
    )
    for i in (2, 7):
        results[i] = results[i].reshape(-1, results[i].shape[3])
    return tuple(results)


def solution(mesh):
    return jax.shard_map(
        functools.partial(per_device, mesh.shape["fs"], mesh.shape["tp"]),
        mesh=mesh,
        in_specs=(
            P("fs", "tp"),
            P("fs", "tp"),
            P("fs", "tp"),
            P("fs", "tp"),
            P(),
            P(),
            P("fs", "tp"),
            P(None, "tp"),
            P(None, "tp"),
            P("fs", "tp"),
            P(None, "tp"),
            P(None, "tp"),
        ),
        out_specs=(
            P("fs", "tp"),
            P("fs", "tp"),
            P(None, "tp"),
            P(None, "tp"),
            P(None, "tp"),
            P("fs", "tp"),
            P("fs", "tp"),
            P(None, "tp"),
            P(None, "tp"),
            P(None, "tp"),
        ),
        check_vma=False,
    )
```

```python
import collections
import functools
import math

import jax
import jax.numpy as jnp
from jax import lax
from jax.experimental import pallas as pl
from jax.experimental.pallas import tpu as pltpu
from jax.sharding import PartitionSpec as P

BETA_ONE = 0.8
BETA_TWO = 0.9
EPSILON = 1e-08
STEP_RATE = 0.005
FLOOR = 0.25

MESH = pl.DeviceIdType.MESH
A, B, UP, DOWN = range(4)
PLANE = 4
GRAIN = 4
LATENCY = 8
LEAD = 4.0
FLIGHT = 0.75


def pieces_of(rows, cols):
    if rows % 64 == 0 and rows * cols * 2 >= 4 * 131072:
        third = rows * 3 // 8 // 16 * 16
        rest = rows * 3 // 4 - third
        return [(0, third), (third, rest), (third + rest, rows - third - rest)], 1
    return [(0, rows)], 0


def classes_of(shapes):
    out = []
    for array, shape in enumerate(shapes):
        ranges, crossing = pieces_of(*shape)
        for p, (start, height) in enumerate(ranges):
            plane_first = p >= len(ranges) - crossing
            flip = A if (p + array) % 2 == 0 else B
            out.append((array, (start, height), plane_first, flip, height / shape[0]))
    return out


def onward(n_z, classes, z, item, via):
    _, fa, fb, p = item
    _, _, plane_first, order, _ = classes[p]
    up = [UP] if z < n_z - 1 else []
    down = [DOWN] if z > 0 else []
    if via is None:
        return [A, B] + up + down
    if via in (UP, DOWN):
        return (up if via == UP else down) + ([] if plane_first else [A, B])
    links = []
    if (fa, fb) == (1, 0) and order == A:
        links.append(B)
    if (fa, fb) == (0, 1) and order == B:
        links.append(A)
    return links + (up + down if plane_first else [])


def hops_left(n_z, classes, z, item, link):
    _, fa, fb, p = item
    _, _, plane_first, order, _ = classes[p]
    if link in (UP, DOWN):
        return (n_z - 2 - z if link == UP else z - 1) + (0 if plane_first else 2)
    turn = 1 if link == order and (fa, fb) == (0, 0) else 0
    return turn + (max(n_z - 1 - z, z) if plane_first else 0)


def plan(n_z, classes, reserved):
    pool = collections.defaultdict(list)
    arriving = collections.defaultdict(list)
    sends = {z: [] for z in range(n_z)}
    takes = {z: [] for z in range(n_z)}
    busy = collections.defaultdict(int)
    for z in range(n_z):
        for p in range(len(classes)):
            item = (z, 0, 0, p)
            for link in onward(n_z, classes, z, item, None):
                pool[z, link].append((0, item))
    missing = n_z * (n_z * PLANE - 1) * len(classes)
    lengths = [max(1, round(4 * GRAIN * x[4])) for x in classes]
    tick = 0
    while missing:
        for z, item, via in arriving.pop(tick, ()):
            for link in onward(n_z, classes, z, item, via):
                pool[z, link].append((tick, item))
        for z in range(n_z):
            toward = 1 if 2 * z < n_z else -1
            for link in range(4):
                held = [
                    n * GRAIN
                    for start, way, n in reserved
                    if way == link and start * GRAIN == tick
                ]
                if held:
                    busy[z, link] = max(tick, busy[z, link]) + held[0]
                waiting = pool[z, link]
                if busy[z, link] > tick or not waiting:
                    continue
                best = max(
                    waiting,
                    key=lambda x: (
                        hops_left(n_z, classes, z, x[1], link),
                        -abs(x[1][0] - z),
                        (x[1][0] - z) * toward,
                        -x[1][3],
                        -x[0],
                        -x[1][1],
                        -x[1][2],
                    ),
                )
                waiting.remove(best)
                item = best[1]
                source, fa, fb, p = item
                sends[z].append((tick, link, item))
                if link == A:
                    there, got = z, (source, 1 - fa, fb, p)
                elif link == B:
                    there, got = z, (source, fa, 1 - fb, p)
                else:
                    there, got = z + (1 if link == UP else -1), item
                takes[there].append((tick, link, got))
                arriving[tick + lengths[p] + (LATENCY - 1) * GRAIN].append((there, got, link))
                busy[z, link] = tick + lengths[p]
                missing -= 1
        tick += 1
    return sends, takes


def mirrored(n_z, events):
    swap = {A: A, B: B, UP: DOWN, DOWN: UP}
    return sorted(
        (tick, swap[link], (n_z - 1 - s, fa, fb, p)) for tick, link, (s, fa, fb, p) in events
    )


def roles_of(n_z, classes, sends, takes):
    pairs = n_z % 2 == 0 and all(
        sorted(x[z]) == mirrored(n_z, x[n_z - 1 - z])
        for x in (sends, takes)
        for z in range(n_z // 2)
    )
    roles = []
    for z in range(n_z // 2 if pairs else n_z):
        events = []
        done = {}
        for tick, link, (source, fa, fb, p) in sorted(takes[z]):
            item = (source - z, fa, fb, p)
            done[item] = tick / GRAIN + 4 * classes[p][4] + FLIGHT
            events.append((done[item], 0, "take", link, item))
        last = collections.defaultdict(float)
        for tick, link, (source, fa, fb, p) in sorted(sends[z]):
            item = (source - z, fa, fb, p)
            at = tick / GRAIN
            when = max(at - LEAD, done.get(item, 0.0), last[link])
            if item not in done and at <= 4:
                when = 0.0
            last[link] = when
            events.append((when, 1, "send", link, item))
            events.append((max(at + 3.0, when + 2.0), 2, "sent", link, item))
        roles.append((sorted(events, key=lambda e: e[:2]), done))
    return pairs, roles


def levels_of(n_z, z):
    near, toward = (z, 1) if 2 * z < n_z else (n_z - 1 - z, -1)
    out = []
    for level in range(n_z):
        step = (level + 1) // 2 if level % 2 else -(level // 2)
        out.append(toward * (step if level <= 2 * near else level - near))
    return out


def level_z(n_z, here_z, level):
    near = jnp.where(2 * here_z < n_z, here_z, n_z - 1 - here_z)
    toward = jnp.where(2 * here_z < n_z, 1, -1)
    step = (level + 1) // 2 if level % 2 else -(level // 2)
    return here_z + toward * jnp.where(level <= 2 * near, step, level - near)


def renew(source_z, factor, high, start, old, out, first):
    _, tall, cols = old.shape
    tile = 512 if cols % 512 == 0 else cols

    def body(c, carry):
        source = source_z * PLANE + c
        here = factor[pl.ds(pl.multiple_of(source * tall, tall), tall), :]
        for t in range(cols // tile):
            at = slice(t * tile, (t + 1) * tile)
            inner = slice(start + t * tile, start + (t + 1) * tile)
            moved = jnp.dot(here, high[:, inner], preferred_element_type=jnp.float32)
            fresh = old[source, :, at].astype(jnp.float32) - STEP_RATE * moved
            out[first + c, :, at] = fresh.astype(jnp.bfloat16)
        return carry

    lax.fori_loop(0, PLANE, body, 0)


def step_kernel(
    n_fs,
    n_tp,
    normed_hbm,
    mixer_hbm,
    value_cot_hbm,
    output_cot_hbm,
    value_factor_hbm,
    output_factor_hbm,
    value_moment_hbm,
    value_second_hbm,
    output_moment_hbm,
    output_second_hbm,
    value_master_hbm,
    output_master_hbm,
    value_step,
    value_new,
    value_all,
    value_moment_new,
    value_second_new,
    output_step,
    output_new,
    output_all,
    output_moment_new,
    output_second_new,
    value_factor,
    output_factor,
    high,
    normed,
    mixer,
    value_cot,
    output_cot,
    value_moment,
    value_second,
    output_moment,
    output_second,
    value_master,
    output_master,
    load_sem,
    master_sem,
    input_ref,
    mixer_ref,
    near_in,
    near_mix,
    squares,
    near_squares,
    total,
    part,
    a_recv,
    b_part,
    b_recv,
    quarter,
    z_part,
    z_recv,
    shares,
    wide,
    low,
    near_send,
    near_recv,
    sum_send,
    sum_recv,
    share_send,
    share_recv,
    gather_send,
    gather_recv,
):
    f32, bf16 = jnp.float32, jnp.bfloat16
    me = lax.axis_index("fs")
    column = lax.axis_index("tp")
    n_z = n_fs // PLANE
    half = n_fs // 2
    here_a = lax.rem(me, 2)
    here_b = lax.rem(me // 2, 2)
    here_z = me // PLANE
    alls = (value_all, output_all)
    rows = total.shape[1]
    cols = (value_cot.shape[1], output_cot.shape[1])
    starts = (0, cols[0])
    classes = classes_of([x.shape[1:] for x in alls])
    fine = len(classes) == 6

    if fine:
        reserved = (
            (4, A, 3),
            (10, B, 2),
            (15, UP, 1),
            (15, DOWN, 1),
            (20, UP, 1),
            (20, DOWN, 1),
            (25, A, 2),
            (30, B, 3),
        )
        stages = (7.8, 12.8, 17.8, 22.8, 27.8, 33.8)
    else:
        reserved = ()
        stages = tuple(7.8 + 4 * i for i in range(6))
    sends, takes = plan(n_z, classes, reserved)
    pairs, roles = roles_of(n_z, classes, sends, takes)
    if pairs:
        toward = jnp.where(2 * here_z < n_z, 1, -1)
        role = jnp.where(2 * here_z < n_z, here_z, n_z - 1 - here_z)
    else:
        toward = 1
        role = here_z

    across_a = me + 1 - 2 * here_a
    across_b = me + 2 - 4 * here_b
    targets = {
        A: across_a,
        B: across_b,
        UP: me + toward * PLANE,
        DOWN: me - toward * PLANE,
    }
    places = {
        (fa, fb): (1 - here_b if fb else here_b) * 2 + (1 - here_a if fa else here_a)
        for fa in range(2)
        for fb in range(2)
    }

    def z_mate(k):
        return lax.rem(here_z + k, n_z) * PLANE + lax.rem(me, PLANE)

    masters = []
    for array, (first, height), _, _, _ in classes:
        hbm, master = ((value_master_hbm, value_master), (output_master_hbm, output_master))[array]
        at = pl.ds(first, height)
        masters.append(
            pltpu.make_async_copy(hbm.at[at], master.at[at], master_sem.at[len(masters)])
        )
    loads = [
        pltpu.make_async_copy(src, dst, load_sem.at[i])
        for i, (src, dst) in enumerate(
            (
                (mixer_hbm, mixer),
                (output_factor_hbm, output_factor),
                (normed_hbm, normed),
                (value_factor_hbm, value_factor),
                (value_cot_hbm, value_cot),
                (output_cot_hbm, output_cot),
                (value_moment_hbm, value_moment),
                (value_second_hbm, value_second),
                (output_moment_hbm, output_moment),
                (output_second_hbm, output_second),
            )
        )
    ]

    opening = [[] for _ in classes]
    for k, (events, _) in enumerate(roles):
        for when, _, kind, link, item in events:
            if kind == "send" and when == 0.0:
                opening[item[3]].append((k, link, item))
    queue = sorted(
        range(len(classes)),
        key=lambda p: min(
            [t for z in sends for t, _, item in sends[z] if item == (z, 0, 0, p)]
        ),
    )
    for p in queue:
        masters[p].start()

    barrier = pltpu.get_barrier_semaphore()
    for there in [across_a, across_b] + [z_mate(k) for k in range(1, n_z)]:
        pl.semaphore_signal(barrier, inc=1, device_id={"fs": there}, device_id_type=MESH)
    for k in range(1, n_tp):
        pl.semaphore_signal(
            barrier,
            inc=1,
            device_id={"tp": lax.rem(column + k, n_tp)},
            device_id_type=MESH,
        )

    def piece_copy(link, item):
        offset, fa, fb, p = item
        source = (here_z + toward * offset) * PLANE + places[fa, fb]
        array, (first, height), _, _, _ = classes[p]
        there = alls[array].at[source, pl.ds(first, height)]
        return pltpu.make_async_remote_copy(
            src_ref=there,
            dst_ref=there,
            send_sem=gather_send.at[link, source, p],
            recv_sem=gather_recv.at[source, p],
            device_id={"fs": targets[link]},
            device_id_type=MESH,
        )

    def open_piece(p):
        for k in range(len(roles)):
            out = [x for x in opening[p] if x[0] == k]
            if out:

                @pl.when(role == k)
                def _(out=out):
                    for _, link, item in out:
                        piece_copy(link, item).start()

    for n, p in enumerate(queue):
        masters[p].wait()
        array, (first, height), _, _, _ = classes[p]
        at = slice(first, first + height)
        master = (value_master, output_master)[array]
        alls[array][me, at, :] = master[at, :].astype(bf16)
        if n == len(queue) - 1:
            for copy in loads:
                copy.start()
        if n == 0:
            pl.semaphore_wait(barrier, 2 + (n_z - 1) + (n_tp - 1))
        else:
            open_piece(queue[n - 1])
    open_piece(queue[-1])

    def run_events(k, first, last):
        events = [
            e for e in roles[k][0] if first <= e[0] < last and (e[2] != "send" or e[0] > 0.0)
        ]
        if not events:
            return

        @pl.when(role == k)
        def _():
            for _, _, kind, link, item in events:
                copy = piece_copy(link, item)
                if kind == "take":
                    copy.wait_recv()
                elif kind == "send":
                    copy.start()
                else:
                    copy.wait_send()

    def message(src, dst, there, sems, index):
        send, recv = sems
        return pltpu.make_async_remote_copy(
            src_ref=src,
            dst_ref=dst,
            send_sem=send.at[index],
            recv_sem=recv.at[index],
            device_id={"fs": there},
            device_id_type=MESH,
        )

    sums = (sum_send, sum_recv)
    shared = (share_send, share_recv)
    pending = []

    def start(copies):
        for copy in copies:
            copy.start()
        pending.extend(copies)
        return copies

    a_sum = message(part.at[pl.ds((1 - here_a) * half, half)], a_recv, across_a, sums, 0)
    b_sum = message(b_part, b_recv, across_b, sums, n_z)
    owners = n_z // 2 if n_z % 4 == 0 else n_z
    edge = (n_z - owners) // 2
    depth = n_z // owners
    mine = here_a * half + here_b * n_z
    is_owner = jnp.logical_and(here_z >= edge, here_z < edge + owners)

    def z_sum(j, k):
        return message(
            z_part.at[pl.ds(j * depth, depth)],
            z_recv.at[k],
            (edge + j) * PLANE + lax.rem(me, PLANE),
            sums,
            k,
        )

    def z_share(j, k):
        at = shares.at[pl.ds(mine + j * depth, depth)]
        return message(at, at, lax.rem(edge + j + k, n_z) * PLANE + lax.rem(me, PLANE), shared, k)
    ours = shares.at[pl.ds(mine, n_z)]
    other = shares.at[pl.ds((1 - here_a) * half + here_b * n_z, n_z)]
    a_share = message(ours, ours, across_a, shared, 0)
    b_shares = [
        message(ours, ours, across_b, shared, n_z),
        message(other, other, across_b, shared, n_z + 1),
    ]

    def products():
        near = []
        for i, (tokens, factor, own, dst) in enumerate(
            (
                (mixer, output_factor, mixer_ref, near_mix),
                (normed, value_factor, input_ref, near_in),
            )
        ):
            loads[2 * i].wait()
            loads[2 * i + 1].wait()
            depth = tokens.shape[1]
            rows_here = factor[pl.ds(pl.multiple_of(column * depth, depth), depth), :]
            own[...] = jnp.dot(
                tokens[...], rows_here, preferred_element_type=f32
            ).astype(bf16)
            for k in range(1, n_tp):
                copy = pltpu.make_async_remote_copy(
                    src_ref=own,
                    dst_ref=dst.at[k - 1],
                    send_sem=near_send.at[k - 1, i],
                    recv_sem=near_recv.at[k - 1, i],
                    device_id={"tp": lax.rem(column + k, n_tp)},
                    device_id_type=MESH,
                )
                copy.start()
                near.append(copy)
        for copy in near:
            copy.wait()
        input_total = input_ref[...].astype(f32)
        mixer_total = mixer_ref[...].astype(f32)
        for k in range(n_tp - 1):
            input_total += near_in[k].astype(f32)
            mixer_total += near_mix[k].astype(f32)
        for copy in loads[4:6]:
            copy.wait()
        across = (((0,), (0,)), ((), ()))
        for i, (left, right) in enumerate(
            (
                (input_total.astype(bf16), value_cot),
                (mixer_total.astype(bf16), output_cot),
            )
        ):
            tile = 512 if cols[i] % 512 == 0 else cols[i]
            for c in range(cols[i] // tile):
                product = lax.dot_general(
                    left,
                    right[:, c * tile : (c + 1) * tile],
                    across,
                    preferred_element_type=f32,
                )
                at = slice(starts[i] + c * tile, starts[i] + (c + 1) * tile)
                for s in range(n_fs):
                    block = product[s * rows : (s + 1) * rows]
                    total[s, :, at] = block
                    part[s, :, at] = block.astype(bf16)
        start([a_sum])

    def second_sum():
        a_sum.wait_recv()
        away = (1 - here_b) * n_z
        b_part[...] = (
            total[pl.ds(here_a * half + away, n_z)] + a_recv[pl.ds(away, n_z)].astype(f32)
        ).astype(bf16)
        start([b_sum])
        quarter[...] = total[pl.ds(mine, n_z)] + a_recv[pl.ds(here_b * n_z, n_z)].astype(f32)

    def third_sum():
        b_sum.wait_recv()
        quarter[...] += b_recv[...].astype(f32)
        z_part[...] = quarter[...].astype(bf16)
        for j in range(owners):

            @pl.when(here_z != edge + j)
            def _(j=j):
                z_sum(j, lax.rem(edge + j - here_z + n_z, n_z)).start()

    def last_sum():
        @pl.when(is_owner)
        def _():
            j = here_z - edge
            done = quarter[pl.ds(j * depth, depth)]
            for k in range(1, n_z):
                z_sum(j, k).wait_recv()
                done += z_recv[k].astype(f32)
            shares[pl.ds(mine + j * depth, depth)] = done.astype(bf16)
            for k in range(1, n_z):
                z_share(j, k).start()

    def share_a():
        for j in range(owners):

            @pl.when(here_z != edge + j)
            def _(j=j):
                z_share(j, lax.rem(here_z - edge - j + n_z, n_z)).wait_recv()

        start([a_share])

    def settle():
        for copy in pending:
            copy.wait_send()
        for j in range(owners):

            @pl.when(here_z != edge + j)
            def _(j=j):
                z_sum(j, lax.rem(edge + j - here_z + n_z, n_z)).wait_send()

        @pl.when(is_owner)
        def _():
            for k in range(1, n_z):
                z_share(here_z - edge, k).wait_send()

    def share_b():
        a_share.wait_recv()
        start(b_shares)

    square_copies = [
        pltpu.make_async_remote_copy(
            src_ref=squares,
            dst_ref=near_squares.at[k - 1],
            send_sem=near_send.at[k - 1, 2],
            recv_sem=near_recv.at[k - 1, 2],
            device_id={"tp": lax.rem(column + k, n_tp)},
            device_id_type=MESH,
        )
        for k in range(1, n_tp)
    ]
    rank = value_factor.shape[1]
    block = 16

    def moments():
        for copy in b_shares:
            copy.wait_recv()
        for copy in loads[6:]:
            copy.wait()
        for s in range(n_fs):
            wide[s * rows : (s + 1) * rows, :] = shares[s].astype(f32)
        for i, (first, second, first_new, second_new) in enumerate(
            (
                (value_moment, value_second, value_moment_new, value_second_new),
                (output_moment, output_second, output_moment_new, output_second_new),
            )
        ):
            span = slice(starts[i], starts[i] + cols[i])

            def body(r, gathered, first=first, second=second, first_new=first_new,
                     second_new=second_new, span=span, i=i):
                at = pl.ds(pl.multiple_of(r * block, block), block)
                projected = wide[at, span]
                m = BETA_ONE * first[at, :] + (1.0 - BETA_ONE) * projected
                v = BETA_TWO * second[at, :] + (1.0 - BETA_TWO) * projected * projected
                norm = m / (jnp.sqrt(v) + EPSILON)
                first_new[at, :] = m
                second_new[at, :] = v
                wide[at, span] = norm
                square = norm * norm
                square = square[:8] + square[8:]
                for c in range(cols[i] // 128):
                    gathered += square[:, c * 128 : (c + 1) * 128]
                return gathered

            squares[i] = lax.fori_loop(
                0, rank // block, body, jnp.zeros((8, 128), f32)
            )
        for copy in square_copies:
            copy.start()

    def steps():
        for copy in square_copies:
            copy.wait()
        for i, (factor, master, step, new) in enumerate(
            (
                (value_factor, value_master, value_step, value_new),
                (output_factor, output_master, output_step, output_new),
            )
        ):
            gathered = squares[i]
            for k in range(n_tp - 1):
                gathered += near_squares[k, i]
            gathered = jnp.sum(jnp.sum(gathered, axis=1, keepdims=True), axis=0, keepdims=True)
            scale = lax.rsqrt(gathered / (rank * cols[i] * n_tp) + FLOOR)
            span = slice(starts[i], starts[i] + cols[i])

            def body(r, carry, span=span, scale=scale, width=cols[i]):
                at = pl.ds(pl.multiple_of(r * block, block), block)
                scaled = wide[at, span] * jnp.broadcast_to(scale, (block, width))
                rounded = scaled.astype(bf16)
                high[at, span] = rounded
                low[at, span] = (scaled - rounded.astype(f32)).astype(bf16)
                return carry

            lax.fori_loop(0, rank // block, body, 0)
            height = master.shape[0]
            here = factor[pl.ds(pl.multiple_of(me * height, height), height), :]
            tile = 512 if cols[i] % 512 == 0 else cols[i]
            for c in range(cols[i] // tile):
                at = slice(c * tile, (c + 1) * tile)
                inner = slice(starts[i] + c * tile, starts[i] + (c + 1) * tile)
                moved = jnp.dot(here, high[:, inner], preferred_element_type=f32) + jnp.dot(
                    here, low[:, inner], preferred_element_type=f32
                )
                step[:, at] = moved
                new[:, at] = master[:, at] - STEP_RATE * moved

    def copies(level, i):
        source_z = level_z(n_z, here_z, level)
        factor = (value_factor, output_factor)[i]
        renew(source_z, factor, high, starts[i], alls[i], alls[i], source_z * PLANE)

    work = [
        (0.5, products),
        (stages[0], second_sum),
        (stages[1], third_sum),
        (stages[2], last_sum),
        (stages[3], share_a),
        (stages[4], share_b),
        (stages[5], moments),
        (stages[5] + 0.5, steps),
        (stages[5] + 4.0, settle),
    ]
    free = stages[5] + 0.6
    ready = []
    for level in range(n_z - 1):
        for i in range(2):
            when = 0.0
            for k in range(len(roles)):
                offset = levels_of(n_z, k)[level]
                for at, _, kind, _, item in roles[k][0]:
                    if item[0] == offset and classes[item[3]][0] == i:
                        when = max(when, at)
            ready.append((when, len(ready), level, i))
    for when, _, level, i in sorted(ready):
        free = max(free + 0.45, when + 0.01)
        work.append((free, functools.partial(copies, level, i)))

    before = -1.0
    for when, action in sorted(work, key=lambda x: x[0]):
        for k in range(len(roles)):
            run_events(k, before, when)
        action()
        before = when
    for k in range(len(roles)):
        run_events(k, before, float("inf"))


def per_device(
    n_fs,
    n_tp,
    normed_input,
    value_cotangent,
    mixer_output,
    output_cotangent,
    value_factor,
    output_factor,
    value_master,
    value_moment,
    value_second,
    output_master,
    output_moment,
    output_second,
):
    f32, bf16 = jnp.float32, jnp.bfloat16
    rank = value_factor.shape[1]
    rows = rank // n_fs
    n_z = n_fs // PLANE
    tokens, value_cols = value_cotangent.shape
    output_cols = output_cotangent.shape[1]
    both = value_cols + output_cols
    others = max(n_tp - 1, 1)
    dma = pltpu.SemaphoreType.DMA
    stacks = []
    for master in (value_master, output_master):
        stacks.append((n_fs,) + master.shape)
    n_pieces = len(classes_of([x[1:] for x in stacks]))
    streamed = (
        normed_input,
        mixer_output,
        value_cotangent,
        output_cotangent,
        value_factor,
        output_factor,
        value_moment,
        value_second,
        output_moment,
        output_second,
        value_master,
        output_master,
    )
    outs = []
    for master, moment, stack in (
        (value_master, value_moment, stacks[0]),
        (output_master, output_moment, stacks[1]),
    ):
        outs += [
            (master.shape, f32),
            (master.shape, f32),
            (stack, bf16),
            (moment.shape, f32),
            (moment.shape, f32),
        ]
    outs += [(value_factor.shape, bf16), (output_factor.shape, bf16), ((rank, both), bf16)]
    room = (62 << 20) - sum(math.prod(x) * jnp.dtype(t).itemsize for x, t in outs)
    held = [x for x in streamed if x is not value_factor and x is not output_factor]
    results = pl.pallas_call(
        functools.partial(step_kernel, n_fs, n_tp),
        out_shape=tuple(pltpu.VMEM(*x) for x in outs),
        in_specs=[pl.BlockSpec(memory_space=pltpu.HBM)] * len(streamed),
        out_specs=(pl.BlockSpec(memory_space=pltpu.VMEM),) * len(outs),
        scratch_shapes=[pltpu.VMEM(x.shape, x.dtype) for x in held]
        + [
            dma((10,)),
            dma((n_pieces,)),
            pltpu.VMEM((tokens, rank), bf16),
            pltpu.VMEM((tokens, rank), bf16),
            pltpu.VMEM((others, tokens, rank), bf16),
            pltpu.VMEM((others, tokens, rank), bf16),
            pltpu.VMEM((2, 8, 128), f32),
            pltpu.VMEM((others, 2, 8, 128), f32),
            pltpu.VMEM((n_fs, rows, both), f32),
            pltpu.VMEM((n_fs, rows, both), bf16),
            pltpu.VMEM((n_fs // 2, rows, both), bf16),
            pltpu.VMEM((n_z, rows, both), bf16),
            pltpu.VMEM((n_z, rows, both), bf16),
            pltpu.VMEM((n_z, rows, both), f32),
            pltpu.VMEM((n_z, rows, both), bf16),
            pltpu.VMEM((n_z, 2 if n_z % 4 == 0 else 1, rows, both), bf16),
            pltpu.VMEM((n_fs, rows, both), bf16),
            pltpu.VMEM((rank, both), f32),
            pltpu.VMEM((rank, both), bf16),
            dma((others, 3)),
            dma((others, 3)),
            dma((n_z + 1,)),
            dma((n_z + 1,)),
            dma((n_z + 2,)),
            dma((n_z + 2,)),
            dma((4, n_fs, n_pieces)),
            dma((n_fs, n_pieces)),
        ],
        compiler_params=pltpu.CompilerParams(
            collective_id=0, has_side_effects=True, vmem_limit_bytes=room
        ),
    )(*streamed)
    return store(n_fs, results)


def store_kernel(n_fs, *refs):
    results, (value_factor, output_factor, high) = refs[:10], refs[10:13]
    outs, last, sem = refs[13:23], refs[23:25], refs[25]
    n_z = n_fs // PLANE
    here_z = lax.axis_index("fs") // PLANE
    copies = []

    def begin(src, dst):
        copy = pltpu.make_async_copy(src, dst, sem.at[len(copies)])
        copy.start()
        copies.append(copy)

    for level in range(n_z - 1):
        at = pl.ds(level_z(n_z, here_z, level) * PLANE, PLANE)
        for i in (2, 7):
            begin(results[i].at[at], outs[i].at[at])
    for i in range(10):
        if i % 5 != 2:
            begin(results[i], outs[i])
    far = level_z(n_z, here_z, n_z - 1)
    start = 0
    for i, factor in enumerate((value_factor, output_factor)):
        old = results[2 + 5 * i]
        renew(far, factor, high, start, old, last[i], 0)
        start += old.shape[2]
        begin(last[i], outs[2 + 5 * i].at[pl.ds(far * PLANE, PLANE)])
    for copy in copies:
        copy.wait()


def store(n_fs, arrays):
    outs = [jax.ShapeDtypeStruct(x.shape, x.dtype) for x in arrays[:10]]
    results = list(
        pl.pallas_call(
            functools.partial(store_kernel, n_fs),
            out_shape=tuple(outs),
            in_specs=[pl.BlockSpec(memory_space=pltpu.VMEM)] * len(arrays),
            out_specs=(pl.BlockSpec(memory_space=pltpu.HBM),) * len(outs),
            scratch_shapes=[
                pltpu.VMEM((PLANE,) + arrays[i].shape[1:], jnp.bfloat16) for i in (2, 7)
            ]
            + [pltpu.SemaphoreType.DMA((2 * (n_fs // PLANE) + 8,))],
            compiler_params=pltpu.CompilerParams(vmem_limit_bytes=6 << 20),
        )(*arrays)
    )
    for i in (2, 7):
        results[i] = results[i].reshape(-1, results[i].shape[2])
    return tuple(results)


def solution(mesh):
    return jax.shard_map(
        functools.partial(per_device, mesh.shape["fs"], mesh.shape["tp"]),
        mesh=mesh,
        in_specs=(
            P("fs", "tp"),
            P("fs", "tp"),
            P("fs", "tp"),
            P("fs", "tp"),
            P(),
            P(),
            P("fs", "tp"),
            P(None, "tp"),
            P(None, "tp"),
            P("fs", "tp"),
            P(None, "tp"),
            P(None, "tp"),
        ),
        out_specs=(
            P("fs", "tp"),
            P("fs", "tp"),
            P(None, "tp"),
            P(None, "tp"),
            P(None, "tp"),
            P("fs", "tp"),
            P("fs", "tp"),
            P(None, "tp"),
            P(None, "tp"),
            P(None, "tp"),
        ),
        check_vma=False,
    )
```
